32 devices in a mesh: dp: 4 (over y, x), kv: 4 (over z), tp: 2 (over core).
Axes of the slice: x: 2, y: 2, z: 4, core: 2. Of those that a mesh axis runs over, the one named last changes fastest.
Arguments:
- tokens: bfloat16 [256, 4096], P('dp', 'kv'), may hold values from -24 to 24
- state: float32 [256, 64, 64, 64], P(('dp', 'kv'), 'tp'), may hold values from -4 to 4
- w_query: bfloat16 [4096, 4096], P('kv', 'tp'), may hold values from -0.09375 to 0.09375
- w_forget: bfloat16 [4096, 4096], P('kv', 'tp'), may hold values from -0.09375 to 0.09375
- w_input: bfloat16 [4096, 4096], P('kv', 'tp'), may hold values from -0.09375 to 0.09375
- w_gate: bfloat16 [4096, 4096], P('kv', 'tp'), may hold values from -0.09375 to 0.09375
- lower_bound: float32 [4096], P('tp'), may hold values from 0 to 0.9
- head_gain: float32 [64], replicated, may hold values from 0.1 to 1.9
- w_out: bfloat16 [4096, 4096], P('tp', 'kv'), may hold values from -0.09375 to 0.09375
- gain_one: float32 [4096], P(('kv', 'tp')), may hold values from 0.1 to 1.9
- bias_one: float32 [4096], P(('kv', 'tp')), may hold values from -2 to 2
- w_up: bfloat16 [4096, 16384], P(None, ('kv', 'tp')), may hold values from -0.09375 to 0.09375
- w_down: bfloat16 [16384, 4096], P(('kv', 'tp')), may hold values from -0.0625 to 0.0625
- gain_two: float32 [4096], P(('kv', 'tp')), may hold values from 0.1 to 1.9
- bias_two: float32 [4096], P(('kv', 'tp')), may hold values from -2 to 2
Outputs:
- result: bfloat16 [256, 4096], P('dp', ('kv', 'tp'))
- new_state: float32 [256, 64, 64, 64], P(('dp', 'kv'), 'tp')
The draws below stay inside these ranges and needn't reach their ends.
All inputs are finite; a program needn't handle non-finite values.
Results may differ from the reference program's by a relative error of at most 0.014.
Values may be sent and summed in bfloat16 or wider, within the bound.
A program may use at most 128 MiB of HBM per device.

```python
import math
import jax
import jax.numpy as jnp
from jax import lax

D = 4096
HEADS = 64
DK = 64
FF = 16384
HW = 4096
BATCH = 256


def draw_tokens(key, part):
    key_base = jax.random.fold_in(key, 11)
    key_scale = jax.random.fold_in(key, 12)
    base = jnp.clip(jax.random.normal(key_base, (BATCH, D), jnp.float32), -8.0, 8.0)
    scales = jnp.exp(jax.random.uniform(key_scale, (16,), jnp.float32, math.log(0.3), math.log(3.0)))
    column_scale = jnp.repeat(scales, D // 16)
    return (base * column_scale[None, :]).astype(jnp.bfloat16)


def spiked(drawn, key, source, target, parts, factor):
    def block_of(dim):
        return (jnp.arange(drawn.shape[dim]) // (drawn.shape[dim] // parts)).reshape((-1,) + (1,) * (drawn.ndim - 1 - dim))

    one_side = jax.random.permutation(key, parts)[block_of(target)]
    far = (block_of(target) + parts // 2) % parts
    return jnp.where((block_of(source) == one_side) | (block_of(source) == far), factor * drawn, drawn)


def shard_levels(rng, shape, shards, smallest, high):
    def one(axis_at, shards_of):
        draws = jax.random.uniform(jax.random.fold_in(jax.random.fold_in(rng, 6), axis_at), (shards_of,), jnp.float32, smallest / len(shards), high / len(shards))
        return jnp.repeat(jnp.exp(draws), shape[axis_at] // shards_of).reshape((-1,) + (1,) * (len(shape) - axis_at - 1))

    loudness = one(*shards[0])
    for cut in shards[1:]:
        loudness = loudness * one(*cut)
    return loudness


def bell_draw(key, dims, scale, most, shards=(), held_as=jnp.bfloat16):
    entries = scale * jax.random.normal(key, dims, jnp.float32)
    if shards:
        entries = entries * shard_levels(key, dims, shards, -0.22, 0.18)
    return jnp.clip(entries, -most, most).astype(held_as)


def heavy_noise(rng, extent, deviation, reach, shards, heavy, kind=jnp.bfloat16):
    values = deviation * jax.random.normal(rng, extent, jnp.float32)
    if shards:
        values = values * shard_levels(rng, extent, shards, -0.22, 0.18)
    return jnp.clip(spiked(values, jax.random.fold_in(rng, 3), *heavy), -reach, reach).astype(kind)


def setup_inputs(seed: int = 0) -> dict:
    splits = jax.random.split(jax.random.key(seed), 16)
    return {
        "tokens": draw_tokens(jax.random.fold_in(splits[15], 71), 0),
        "state": bell_draw(splits[1], (BATCH, HEADS, DK, DK), 0.3, 4.0, ((0, 16), (1, 2)), jnp.float32),
        "w_query": bell_draw(splits[2], (D, HW), D ** -0.5, 0.09375, ((0, 4), (1, 2))),
        "w_forget": bell_draw(splits[3], (D, HW), D ** -0.5, 0.09375, ((0, 4), (1, 2))),
        "w_input": bell_draw(splits[4], (D, HW), D ** -0.5, 0.09375, ((0, 4), (1, 2))),
        "w_gate": bell_draw(splits[5], (D, HW), D ** -0.5, 0.09375, ((0, 4), (1, 2))),
        "lower_bound": jnp.clip(0.9 * jax.random.uniform(splits[6], (HW,), jnp.float32) ** shard_levels(splits[6], (HW,), ((0, 2),), -0.2, 0.2), 0.0, 0.9),
        "head_gain": jnp.clip(1.0 + 0.18 * jax.random.normal(splits[7], (DK,), jnp.float32), 0.1, 1.9),
        "w_out": bell_draw(splits[8], (HW, D), HW ** -0.5, 0.09375, ((0, 2), (1, 4))),
        "gain_one": jnp.clip(1.0 + 0.18 * jax.random.normal(splits[9], (D,), jnp.float32), 0.1, 1.9),
        "bias_one": bell_draw(splits[10], (D,), 0.3, 2.0, ((0, 8),), jnp.float32),
        "w_up": bell_draw(splits[11], (D, FF), D ** -0.5, 0.09375, ((1, 8),)),
        "w_down": heavy_noise(splits[12], (FF, D), FF ** -0.5, 0.0625, ((0, 8),), (0, 1, 8, 2.0)),
        "gain_two": jnp.clip(1.0 + 0.18 * jax.random.normal(splits[13], (D,), jnp.float32), 0.1, 1.9),
        "bias_two": bell_draw(splits[14], (D,), 0.3, 2.0, ((0, 8),), jnp.float32),
    }


epsilon = 0.1
residual_scale = 1.68

def layer_norm(values, gain, bias):
    center = lax.optimization_barrier(jnp.mean(values, axis=-1, keepdims=True))
    spread = lax.optimization_barrier(jnp.mean(jnp.square(values - center), axis=-1, keepdims=True))
    return (values - center) * lax.rsqrt(spread + epsilon) * gain + bias

def project(tokens, weight):
    rounded = jnp.dot(tokens, weight, preferred_element_type=jnp.float32).astype(jnp.bfloat16)
    rounded = lax.optimization_barrier(rounded)
    return rounded.astype(jnp.float32)

def reference(tokens, state, w_query, w_forget, w_input, w_gate, lower_bound, head_gain, w_out, gain_one, bias_one, w_up, w_down, gain_two, bias_two):
    batch = tokens.shape[0]
    shape = (batch, HEADS, DK)
    query_raw = project(tokens, w_query).reshape(shape)
    forget_raw = project(tokens, w_forget).reshape(shape)
    value_raw = project(tokens, w_input).reshape(shape)
    gate_raw = project(tokens, w_gate).reshape(shape)
    bound = lower_bound.reshape(HEADS, DK)
    forget = bound + (1.0 - bound) * jax.nn.sigmoid(forget_raw)
    keyvec = (1.0 - bound) * jax.nn.sigmoid(-forget_raw)
    query = jax.nn.silu(query_raw)
    new_state = forget[..., None] * state + keyvec[..., None] * value_raw[:, :, None, :]
    read = jnp.einsum('bhij,bhi->bhj', new_state, query, precision=lax.Precision.HIGHEST)
    read = read * lax.rsqrt(lax.optimization_barrier(jnp.mean(jnp.square(read), axis=-1, keepdims=True)) + epsilon)
    mixout = (read * head_gain * jax.nn.silu(gate_raw)).reshape(batch, HEADS * DK).astype(jnp.bfloat16)
    mixed = jnp.dot(mixout, w_out, preferred_element_type=jnp.float32)
    first = residual_scale * tokens.astype(jnp.float32) + mixed
    normed = layer_norm(first, gain_one, bias_one).astype(jnp.bfloat16)
    upper = jnp.dot(normed, w_up, preferred_element_type=jnp.float32)
    hidden = jnp.square(jax.nn.relu(upper)).astype(jnp.bfloat16)
    mlp = jnp.dot(hidden, w_down, preferred_element_type=jnp.float32)
    second = residual_scale * normed.astype(jnp.float32) + mlp
    result = layer_norm(second, gain_two, bias_two).astype(jnp.bfloat16)
    return (result, new_state)
```

```python
import functools
import types

import jax
import jax.numpy as jnp
import numpy as np
from jax import lax
from jax.experimental import pallas as pl
from jax.experimental.pallas import tpu as pltpu
from jax.sharding import PartitionSpec as P

epsilon = 0.1
residual_scale = 1.68
MESH = pl.DeviceIdType.MESH
LAYER_BYTES = 47 * 1024 * 1024
WRITE_BYTES = 1024 * 1024


def shifted(index, by, count):
    return lax.rem(index + by, count)


def greet(peers):
    barrier = pltpu.get_barrier_semaphore()
    for peer in peers:
        pl.semaphore_signal(barrier, inc=1, device_id=peer, device_id_type=MESH)
    return lambda: pl.semaphore_wait(barrier, len(peers))


def send(source, target, send_sem, recv_sem, peer):
    copy = pltpu.make_async_remote_copy(
        src_ref=source,
        dst_ref=target,
        send_sem=send_sem,
        recv_sem=recv_sem,
        device_id=peer,
        device_id_type=MESH,
    )
    copy.start()
    return copy


def store(source, target, sem):
    copy = pltpu.make_async_copy(source, target, sem)
    copy.start()
    return copy


def to_lanes(column):
    count = column.shape[0]
    diagonal = lax.broadcasted_iota(jnp.int32, (count, count), 0) == lax.broadcasted_iota(
        jnp.int32, (count, count), 1
    )
    return jnp.sum(jnp.where(diagonal, column, 0.0), axis=0, keepdims=True)


def to_sublanes(row):
    count = row.shape[1]
    diagonal = lax.broadcasted_iota(jnp.int32, (count, count), 0) == lax.broadcasted_iota(
        jnp.int32, (count, count), 1
    )
    return jnp.sum(jnp.where(diagonal, row, 0.0), axis=1, keepdims=True)


def pick_matrix(rows, lanes):
    depth, width = 4 * rows, rows * 2 * lanes
    line = lax.broadcasted_iota(jnp.int32, (depth, width), 0)
    lane = lax.broadcasted_iota(jnp.int32, (depth, width), 1)
    same_row = lax.rem(line, rows) == lax.div(lane, 2 * lanes)
    same_half = (line < 2 * rows) == (lax.rem(lane, 2 * lanes) < lanes)
    return jnp.where(same_row & same_half, 1.0, 0.0).astype(jnp.bfloat16)


def layer_kernel(n, t, size, names, *refs):
    r = types.SimpleNamespace(**dict(zip(names, refs)))
    kv, tp = lax.axis_index("kv"), lax.axis_index("tp")
    count, columns = r.out.shape
    rows = count // n
    group = n * t
    me = kv * t + tp
    width = group * columns
    groups, kinds, _, _, wide = r.whole.shape
    heads = wide // size
    lanes = 2 * size
    pieces = r.down.shape[0] // group
    depth_down = r.down.shape[1]
    offsets = [(o, u) for o in range(n) for u in range(t) if (o, u) != (0, 0)]
    relay = n >= 4
    last = n - 1

    def at(o, u):
        return {"kv": shifted(kv, o, n), "tp": shifted(tp, u, t)}

    def block(o, u):
        return shifted(kv, o, n) * t + shifted(tp, u, t)

    def columns_of(index):
        return pl.ds(pl.multiple_of(index * columns, columns), columns)

    wait_barrier = greet([at(o, u) for o, u in offsets])

    small = [
        store(source, target, r.small_sem.at[i])
        for i, (source, target) in enumerate(
            [
                (r.tokens_in, r.tokens),
                (r.bound_in, r.bound),
                (r.gain_in, r.gain),
                (r.gain_one_in, r.gain_one),
                (r.bias_one_in, r.bias_one),
                (r.gain_two_in, r.gain_two),
                (r.bias_two_in, r.bias_two),
            ]
        )
    ]
    weights = (r.w_query, r.w_forget, r.w_input, r.w_gate)
    loads = {
        (j, w): store(
            weights[w].at[:, pl.ds(j * wide, wide)],
            r.pool.at[j * kinds + w],
            r.load_project.at[j * kinds + w],
        )
        for j in range(groups)
        for w in range(kinds)
    }

    r.pick[...] = pick_matrix(rows, lanes)
    if relay:

        @pl.when(kv == 0)
        def _():
            for j in range(groups):
                r.got[j, 0] = jnp.zeros(r.got.shape[2:], jnp.bfloat16)

        @pl.when(kv == last)
        def _():
            for j in range(groups):
                r.got[j, last - 1] = jnp.zeros(r.got.shape[2:], jnp.bfloat16)

    def guarded(condition, action):
        if condition is None:
            action()
        else:
            pl.when(condition)(action)

    sends = {}

    def direct(j, o):
        return pltpu.make_async_remote_copy(
            src_ref=r.sent.at[j, shifted(kv, o, n)],
            dst_ref=r.got.at[j, o - 1],
            send_sem=r.sum_send.at[j, o - 1],
            recv_sem=r.sum_recv.at[j, o - 1],
            device_id=at(o, 0),
            device_id_type=MESH,
        )

    def sends_direct(o):
        condition = None
        if relay:
            terms = []
            if o == 1:
                terms.append(kv != last)
            if o == last:
                terms.append(kv != 0)
            if o == last - 1:
                terms.append(kv != 1)
            if o == 2:
                terms.append(kv != last - 1)
            for term in terms:
                condition = term if condition is None else condition & term
        return condition

    def receives(o):
        if relay and o == 1:
            return kv != 0
        if relay and o == last:
            return kv != last
        return None

    is_end = (kv == 0) | (kv == last)
    is_relay = (kv == 1) | (kv == last - 1)

    def to_relay(j):
        return pltpu.make_async_remote_copy(
            src_ref=r.sent.at[j, last - kv],
            dst_ref=r.relay_got.at[j],
            send_sem=r.relay_send.at[j],
            recv_sem=r.relay_recv.at[j],
            device_id={"kv": 1 + (kv // last) * (last - 2), "tp": tp},
            device_id_type=MESH,
        )

    def from_relay(j):
        side = (kv - 1) // (last - 2)
        end = last - last * side
        slot = (last - 2) - (last - 3) * side
        return end, pltpu.make_async_remote_copy(
            src_ref=r.relay_sent.at[j],
            dst_ref=r.got.at[j, slot],
            send_sem=r.relay_send.at[j],
            recv_sem=r.sum_recv.at[j, slot],
            device_id={"kv": end, "tp": tp},
            device_id_type=MESH,
        )

    def project(j):
        for w in range(kinds):
            loads[j, w].wait()
            value = jnp.dot(
                r.tokens[...], r.pool[j * kinds + w], preferred_element_type=jnp.float32
            ).reshape(n, rows, wide)
            r.whole[j, w] = value
            r.sent[j, :, w] = value.astype(jnp.bfloat16)

    def send_far(j):
        if relay:
            pl.when(is_end)(lambda: to_relay(j).start())

    def send_near(j):
        for o in sorted(range(1, n), key=lambda o: -min(o, n - o)):
            guarded(sends_direct(o), lambda o=o: direct(j, o).start())

    def pass_relay(j):
        if not relay:
            return

        @pl.when(is_relay)
        def _():
            to_relay(j).wait_recv()
            end, copy = from_relay(j)
            for w in range(kinds):
                total = r.whole[j, w, end] + r.relay_got[j, w].astype(jnp.float32)
                r.relay_sent[j, w] = total.astype(jnp.bfloat16)
            copy.start()

    def finish_sends(j):
        for o in range(1, n):
            guarded(sends_direct(o), lambda o=o: direct(j, o).wait_send())
        if relay:
            pl.when(is_end)(lambda: to_relay(j).wait_send())
            pl.when(is_relay)(lambda: from_relay(j)[1].wait_send())

    def load_state(j):
        part = pl.ds(j * heads, heads)
        return store(r.state.at[:, part], r.new_state.at[:, part], r.load_state.at[j])

    pending = []

    def update(j):
        for o in range(1, n):
            guarded(receives(o), lambda o=o: direct(j, o).wait_recv())

        def summed(w):
            total = r.whole[j, w, kv]
            for o in range(1, n):
                total = total + r.got[j, o - 1, w].astype(jnp.float32)
            return total.astype(jnp.bfloat16).astype(jnp.float32)

        query_raw, forget_raw, value, gate = (summed(w) for w in range(kinds))
        low = r.bound[:, j * wide : (j + 1) * wide]
        forget = low + (1.0 - low) * jax.nn.sigmoid(forget_raw)
        query = query_raw * jax.nn.sigmoid(query_raw)
        stacked = []
        for factor in (forget, query):
            high = factor.astype(jnp.bfloat16).astype(jnp.float32)
            stacked += [high, factor - high]
        turned = jnp.concatenate(stacked, axis=0).T.reshape(heads, size, 4 * rows)
        r.factors[...] = turned.astype(jnp.bfloat16)
        for h in range(heads):
            pair = value[:, (h // 2) * lanes : (h // 2 + 1) * lanes]
            r.value[h] = pltpu.roll(pair, size, 1) if h % 2 else pair
        r.gate[...] = gate * jax.nn.sigmoid(gate)
        state_loads[j].wait()

        def one_head(h, slot):
            r.spread[slot] = jnp.dot(
                r.factors[h], r.pick[...], preferred_element_type=jnp.float32
            )
            for b in range(rows):
                base = b * 2 * lanes
                line = r.value[h, b : b + 1, :size]
                keep = r.spread[slot, :, base : base + size]
                query_column = r.spread[slot, :, base + lanes : base + lanes + size]
                updated = line + keep * (r.new_state[b, j * heads + h] - line)
                r.new_state[b, j * heads + h] = updated
                r.read[h, b : b + 1] = jnp.sum(updated * query_column, axis=0, keepdims=True)

        def two_heads(i, carry):
            for slot in range(2):
                one_head(i * 2 + slot, slot)
            return carry

        lax.fori_loop(0, heads // 2, two_heads, 0)

        def normalized(h):
            whole = r.read[h]
            return whole * lax.rsqrt(jnp.mean(whole * whole, axis=1, keepdims=True) + epsilon)

        for p in range(heads // 2):
            here = slice(p * lanes, (p + 1) * lanes)
            pair = jnp.concatenate([normalized(2 * p), normalized(2 * p + 1)], axis=1)
            gated = pair * r.gain[...] * r.gate[:, here]
            r.gathered[j, kv, :, here] = gated.astype(jnp.bfloat16)
        for o in range(1, n):
            mixes[j, o] = send(
                r.gathered.at[j, kv],
                r.gathered.at[j, kv],
                r.mix_send.at[j, o],
                r.mix_recv.at[j, o],
                at(o, 0),
            )
            pending.append(mixes[j, o])

    mixes = {}

    def project_out(j):
        for o in range(1, n):
            mixes[j, o].wait_recv()
        whole = r.gathered[j].reshape(count, wide)
        for u in range(t):
            if j == 0:
                loads_out[u].wait()
            product = jnp.dot(
                whole,
                r.out_buf[u, j * wide : (j + 1) * wide],
                preferred_element_type=jnp.float32,
            )
            r.mixed[u] = product if j == 0 else r.mixed[u] + product

    small[0].wait()
    state_loads = {}
    for j in range(groups):
        project(j)
        if j == 0:
            wait_barrier()
        send_far(j)
        send_near(j)
        state_loads[j] = load_state(j)
    for copy in small[1:]:
        copy.wait()
    loads_out = [
        store(r.w_out.at[:, columns_of(shifted(tp, u, t))], r.out_buf.at[u], r.load_out.at[u])
        for u in range(t)
    ]
    up_chunks, _, up_width = r.up_buf.shape
    loads_up = [
        store(r.w_up.at[:, pl.ds(c * up_width, up_width)], r.up_buf.at[c], r.load_up.at[c])
        for c in range(up_chunks)
    ]
    steps = [*range(1, n), 0]
    loads_down = {}
    for s in range(n):
        for u in [*range(1, t), 0]:
            for p in range(pieces):
                slot = (s * t + u) * pieces + p
                loads_down[s, u, p] = store(
                    r.w_down.at[pl.ds(p * depth_down, depth_down), columns_of(block(steps[s], u))],
                    r.down.at[slot],
                    r.load_down.at[slot],
                )

    r.affine[me, 0:1] = r.gain_one[...]
    r.affine[me, 1:2] = r.bias_one[...]
    affines = [
        send(
            r.affine.at[me], r.affine.at[me], r.affine_send.at[o, u], r.affine_recv.at[o, u], at(o, u)
        )
        for o, u in offsets
    ]
    pending += affines

    for j in range(groups):
        pass_relay(j)
        update(j)
        if j:
            project_out(j - 1)
    project_out(groups - 1)

    parts = []
    for u in range(1, t):
        parts.append(
            send(
                r.mixed.at[u],
                r.part_got.at[u - 1],
                r.part_send.at[u],
                r.part_recv.at[u],
                at(0, u),
            )
        )
    pending += parts
    own_tokens = r.tokens[:, columns_of(tp)].astype(jnp.float32)
    first = residual_scale * own_tokens + r.mixed[0]
    for u in range(1, t):
        parts[u - 1].wait_recv()
        first = first + r.part_got[u - 1]
    r.firsts[me] = first.astype(jnp.bfloat16)

    def pass_on(index, o, u):
        where = at(o, u) if u == 0 else at(0, u)
        copy = send(
            r.firsts.at[index], r.firsts.at[index], r.first_send.at[o, u], r.first_recv.at[o, u], where
        )
        pending.append(copy)
        return copy

    passed = {}
    for o in range(1, n):
        passed[o, 0] = pass_on(me, o, 0)
    for u in range(1, t):
        passed[0, u] = pass_on(me, 0, u)
    for copy in affines:
        copy.wait_recv()
    for o in range(1, n):
        passed[o, 0].wait_recv()
        for u in range(1, t):
            passed[o, u] = pass_on(block(n - o, 0), o, u)
    for o in range(n):
        for u in range(1, t):
            passed[o, u].wait_recv()

    total = jnp.zeros((count, 1), jnp.float32)
    for g in range(group):
        total = total + jnp.sum(r.firsts[g].astype(jnp.float32), axis=1, keepdims=True)
    center = total / width
    spread = jnp.zeros((count, 1), jnp.float32)
    for g in range(group):
        away = r.firsts[g].astype(jnp.float32) - center
        spread = spread + jnp.sum(away * away, axis=1, keepdims=True)
    scale = lax.rsqrt(spread / width + epsilon)

    def finish(values, pair):
        return ((values.astype(jnp.float32) - center) * scale * pair[0:1] + pair[1:2]).astype(
            jnp.bfloat16
        )

    for g in range(group):
        r.normed[:, g * columns : (g + 1) * columns] = finish(r.firsts[g], r.affine[g])
    own_normed = finish(r.firsts[me], r.affine[me])

    for c in range(up_chunks):
        loads_up[c].wait()
        upper = jnp.dot(r.normed[...], r.up_buf[c], preferred_element_type=jnp.float32)
        upper = jnp.maximum(upper, 0.0)
        r.hidden[:, c * up_width : (c + 1) * up_width] = (upper * upper).astype(jnp.bfloat16)

    near = {}
    far = {}

    def near_sum(s):
        value = r.kept[s]
        for u in range(1, t):
            near[s, u].wait_recv()
            value = value + r.near_got[s, u - 1].astype(jnp.float32)
        return value

    def far_out(s):
        r.far_sent[s] = near_sum(s).astype(jnp.bfloat16)
        far[s] = send(
            r.far_sent.at[s], r.far_got.at[s], r.far_send.at[s], r.far_recv.at[s], at(steps[s], 0)
        )

    for s in range(n):
        for u in [*range(1, t), 0]:
            product = jnp.zeros((count, columns), jnp.float32)
            for p in range(pieces):
                loads_down[s, u, p].wait()
                product = product + jnp.dot(
                    r.hidden[:, p * depth_down : (p + 1) * depth_down],
                    r.down[(s * t + u) * pieces + p],
                    preferred_element_type=jnp.float32,
                )
            if u:
                r.near_sent[s, u - 1] = product.astype(jnp.bfloat16)
                near[s, u] = send(
                    r.near_sent.at[s, u - 1],
                    r.near_got.at[s, u - 1],
                    r.near_send.at[s, u - 1],
                    r.near_recv.at[s, u - 1],
                    at(0, u),
                )
            else:
                r.kept[s] = product
        if s:
            far_out(s - 1)
    second = residual_scale * own_normed.astype(jnp.float32) + near_sum(n - 1)
    for s in range(n - 1):
        far[s].wait_recv()
        second = second + r.far_got[s].astype(jnp.float32)
    pending += list(near.values()) + list(far.values())

    sums = jnp.concatenate(
        [
            to_lanes(jnp.sum(second, axis=1, keepdims=True)),
            to_lanes(jnp.sum(second * second, axis=1, keepdims=True)),
        ],
        axis=0,
    )
    r.stats[0, 0:2] = sums
    tallies = []
    for i, (o, u) in enumerate(offsets):
        tallies.append(
            send(r.stats.at[0], r.stats.at[i + 1], r.stats_send.at[i], r.stats_recv.at[i], at(o, u))
        )
    pending += tallies
    for i, copy in enumerate(tallies):
        copy.wait_recv()
        sums = sums + r.stats[i + 1, 0:2]
    center_two = to_sublanes(sums[0:1]) / width
    spread_two = to_sublanes(sums[1:2]) / width - center_two * center_two
    result = (second - center_two) * lax.rsqrt(spread_two + epsilon)
    r.out[...] = (result * r.gain_two[...] + r.bias_two[...]).astype(jnp.bfloat16)
    for j in range(groups):
        finish_sends(j)
    for copy in pending:
        copy.wait_send()


def layer(n, t, tokens, state, weights, bound, gain, w_out, w_up, w_down, affine):
    count, depth = tokens.shape
    rows = count // n
    width = weights[0].shape[1]
    kinds = len(weights)
    size = state.shape[3]
    lanes = 2 * size
    wide = min(width, 8 * size)
    groups = width // wide
    heads = wide // size
    columns = affine[0].shape[1]
    model, units = w_up.shape
    group = n * t
    up_width = min(units, 512)
    dma = pltpu.SemaphoreType.DMA
    vmem = pltpu.VMEM
    few, many = jnp.bfloat16, jnp.float32
    shares = columns == wide and units % depth == 0 and group * (units // depth) == groups * kinds
    pieces = units // depth if shares else 1
    inputs = {
        "tokens_in": tokens,
        "state": state,
        "w_query": weights[0],
        "w_forget": weights[1],
        "w_input": weights[2],
        "w_gate": weights[3],
        "bound_in": bound,
        "gain_in": gain,
        "w_out": w_out,
        "w_up": w_up,
        "w_down": w_down,
        "gain_one_in": affine[0],
        "bias_one_in": affine[1],
        "gain_two_in": affine[2],
        "bias_two_in": affine[3],
    }
    scratch = {
        "tokens": vmem(tokens.shape, few),
        "bound": vmem(bound.shape, many),
        "gain": vmem(gain.shape, many),
        "gain_one": vmem((1, columns), many),
        "bias_one": vmem((1, columns), many),
        "gain_two": vmem((1, columns), many),
        "bias_two": vmem((1, columns), many),
        "pool": vmem((groups * kinds, depth, wide), few),
        "whole": vmem((groups, kinds, n, rows, wide), many),
        "sent": vmem((groups, n, kinds, rows, wide), few),
        "got": vmem((groups, n - 1, kinds, rows, wide), few),
        "relay_got": vmem((groups, kinds, rows, wide), few),
        "relay_sent": vmem((groups, kinds, rows, wide), few),
        "pick": vmem((4 * rows, rows * 2 * lanes), few),
        "factors": vmem((heads, size, 4 * rows), few),
        "value": vmem((heads, rows, lanes), many),
        "gate": vmem((rows, wide), many),
        "spread": vmem((2, size, rows * 2 * lanes), many),
        "read": vmem((heads, rows, size), many),
        "gathered": vmem((groups, n, rows, wide), few),
        "out_buf": vmem((t, width, columns), few),
        "mixed": vmem((t, count, columns), many),
        "up_buf": vmem((units // up_width, model, up_width), few),
        "part_got": vmem((t - 1, count, columns), many),
        "affine": vmem((group, 2, columns), many),
        "firsts": vmem((group, count, columns), few),
        "normed": vmem((count, model), few),
        "hidden": vmem((count, units), few),
        "near_sent": vmem((n, t - 1, count, columns), few),
        "near_got": vmem((n, t - 1, count, columns), few),
        "kept": vmem((n, count, columns), many),
        "far_sent": vmem((n, count, columns), few),
        "far_got": vmem((n, count, columns), few),
        "stats": vmem((group, 8, count), many),
        "small_sem": dma((7,)),
        "load_project": dma((groups * kinds,)),
        "load_state": dma((groups,)),
        "load_out": dma((t,)),
        "load_up": dma((units // up_width,)),
        "load_down": dma((group * pieces,)),
        "sum_send": dma((groups, n - 1)),
        "sum_recv": dma((groups, n - 1)),
        "relay_send": dma((groups,)),
        "relay_recv": dma((groups,)),
        "mix_send": dma((groups, n)),
        "mix_recv": dma((groups, n)),
        "part_send": dma((t,)),
        "part_recv": dma((t,)),
        "affine_send": dma((n, t)),
        "affine_recv": dma((n, t)),
        "first_send": dma((n, t)),
        "first_recv": dma((n, t)),
        "near_send": dma((n, t)),
        "near_recv": dma((n, t)),
        "far_send": dma((n,)),
        "far_recv": dma((n,)),
        "stats_send": dma((group,)),
        "stats_recv": dma((group,)),
    }
    if not shares:
        scratch["down"] = vmem((group, units, columns), few)

    def kernel(*refs):
        names = [*inputs, "out", "new_state", *scratch]
        if shares:
            names.append("down")
            refs = (*refs, refs[names.index("pool")])
        layer_kernel(n, t, size, names, *refs)

    return pl.pallas_call(
        kernel,
        out_shape=(vmem((count, columns), few), vmem(state.shape, many)),
        in_specs=[pl.BlockSpec(memory_space=pl.ANY)] * len(inputs),
        out_specs=(pl.BlockSpec(memory_space=pltpu.VMEM),) * 2,
        scratch_shapes=list(scratch.values()),
        compiler_params=pltpu.CompilerParams(
            collective_id=0, has_side_effects=True, vmem_limit_bytes=LAYER_BYTES
        ),
        name="layer",
    )(*inputs.values())


def write_kernel(result, new_state, result_out, state_out, sem):
    pieces = sem.shape[0] - 1
    heads = new_state.shape[1] // pieces
    copies = [store(result, result_out, sem.at[pieces])]
    for i in range(pieces):
        part = pl.ds(i * heads, heads)
        copies.append(store(new_state.at[:, part], state_out.at[:, part], sem.at[i]))
    for copy in copies:
        copy.wait()


def write_out(result, new_state):
    return pl.pallas_call(
        write_kernel,
        out_shape=(
            jax.ShapeDtypeStruct(result.shape, result.dtype),
            jax.ShapeDtypeStruct(new_state.shape, new_state.dtype),
        ),
        in_specs=[pl.BlockSpec(memory_space=pltpu.VMEM)] * 2,
        out_specs=(pl.BlockSpec(memory_space=pl.ANY),) * 2,
        scratch_shapes=[pltpu.SemaphoreType.DMA((9,))],
        compiler_params=pltpu.CompilerParams(vmem_limit_bytes=WRITE_BYTES),
        name="write",
    )(result, new_state)


def per_device(
    tokens,
    state,
    w_query,
    w_forget,
    w_input,
    w_gate,
    lower_bound,
    head_gain,
    w_out,
    gain_one,
    bias_one,
    w_up,
    w_down,
    gain_two,
    bias_two,
):
    n, t = lax.axis_size("kv"), lax.axis_size("tp")
    result, new_state = layer(
        n,
        t,
        tokens,
        state,
        (w_query, w_forget, w_input, w_gate),
        lower_bound[None, :],
        jnp.tile(head_gain, 2)[None, :],
        w_out,
        w_up,
        w_down,
        [vector[None, :] for vector in (gain_one, bias_one, gain_two, bias_two)],
    )
    return write_out(result, new_state)


def solution(mesh):
    placed = (
        P("dp", "kv"),
        P(("dp", "kv"), "tp", None, None),
        P("kv", "tp"),
        P("kv", "tp"),
        P("kv", "tp"),
        P("kv", "tp"),
        P("tp"),
        P(),
        P("tp", "kv"),
        P(("kv", "tp")),
        P(("kv", "tp")),
        P(None, ("kv", "tp")),
        P(("kv", "tp"), None),
        P(("kv", "tp")),
        P(("kv", "tp")),
    )
    return jax.shard_map(
        per_device,
        mesh=mesh,
        in_specs=placed,
        out_specs=(P("dp", ("kv", "tp")), P(("dp", "kv"), "tp", None, None)),
        check_vma=False,
    )
```

```python
import functools
import types

import jax
import jax.numpy as jnp
import numpy as np
from jax import lax
from jax.experimental import pallas as pl
from jax.experimental.pallas import tpu as pltpu
from jax.sharding import PartitionSpec as P

epsilon = 0.1
residual_scale = 1.68
MESH = pl.DeviceIdType.MESH
LAYER_BYTES = 47 * 1024 * 1024
WRITE_BYTES = 1024 * 1024


def shifted(index, by, count):
    return lax.rem(index + by, count)


def greet(peers):
    barrier = pltpu.get_barrier_semaphore()
    for peer in peers:
        pl.semaphore_signal(barrier, inc=1, device_id=peer, device_id_type=MESH)
    return lambda: pl.semaphore_wait(barrier, len(peers))


def send(source, target, send_sem, recv_sem, peer):
    copy = pltpu.make_async_remote_copy(
        src_ref=source,
        dst_ref=target,
        send_sem=send_sem,
        recv_sem=recv_sem,
        device_id=peer,
        device_id_type=MESH,
    )
    copy.start()
    return copy


def store(source, target, sem):
    copy = pltpu.make_async_copy(source, target, sem)
    copy.start()
    return copy


def to_lanes(column):
    count = column.shape[0]
    diagonal = lax.broadcasted_iota(jnp.int32, (count, count), 0) == lax.broadcasted_iota(
        jnp.int32, (count, count), 1
    )
    return jnp.sum(jnp.where(diagonal, column, 0.0), axis=0, keepdims=True)


def to_sublanes(row):
    count = row.shape[1]
    diagonal = lax.broadcasted_iota(jnp.int32, (count, count), 0) == lax.broadcasted_iota(
        jnp.int32, (count, count), 1
    )
    return jnp.sum(jnp.where(diagonal, row, 0.0), axis=1, keepdims=True)


def fill_pick(pick, rows, lanes):
    shape = (4 * rows, 2 * lanes)
    line = lax.broadcasted_iota(jnp.int32, shape, 0)
    lane = lax.broadcasted_iota(jnp.int32, shape, 1)
    same_half = (line < 2 * rows) == (lane < lanes)
    row = lax.rem(line, rows)
    for b in range(rows):
        chosen = jnp.where(same_half & (row == b), 1.0, 0.0)
        pick[:, b * 2 * lanes : (b + 1) * 2 * lanes] = chosen.astype(jnp.bfloat16)


def layer_kernel(n, t, size, names, *refs):
    r = types.SimpleNamespace(**dict(zip(names, refs)))
    kv, tp = lax.axis_index("kv"), lax.axis_index("tp")
    count, columns = r.out.shape
    rows = count // n
    group = n * t
    me = kv * t + tp
    width = group * columns
    groups, kinds, _, _, wide = r.whole.shape
    heads = wide // size
    lanes = 2 * size
    pieces = r.down.shape[0] // group
    depth_down = r.down.shape[1]
    offsets = [(o, u) for o in range(n) for u in range(t) if (o, u) != (0, 0)]
    relay = n == 4
    buddy = kv + 1 - 2 * lax.rem(kv, 2)

    def at(o, u):
        return {"kv": shifted(kv, o, n), "tp": shifted(tp, u, t)}

    def block(o, u):
        return shifted(kv, o, n) * t + shifted(tp, u, t)

    arrivals = sorted(range(1, n), key=lambda o: min(o, n - o))
    if relay:
        arrivals = [2, 3 - 2 * (kv // 2), 1 + 2 * (kv // 2)]

    def columns_of(index):
        return pl.ds(pl.multiple_of(index * columns, columns), columns)

    barrier = pltpu.get_barrier_semaphore()

    def greet_all():
        for o, u in offsets:
            pl.semaphore_signal(barrier, inc=1, device_id=at(o, u), device_id_type=MESH)

    def wait_barrier():
        pl.semaphore_wait(barrier, len(offsets))

    small = []

    def load_small(pairs):
        for source, target in pairs:
            small.append(store(source, target, r.small_sem.at[len(small)]))

    weights = (r.w_query, r.w_forget, r.w_input, r.w_gate)
    loads = {}

    def load_weights(j):
        for w in range(kinds):
            loads[j, w] = store(
                weights[w].at[:, pl.ds(j * wide, wide)],
                r.pool.at[j * kinds + w],
                r.load_project.at[j * kinds + w],
            )

    def wait_tokens():
        small[0].wait()

    def fill():
        fill_pick(r.pick, rows, lanes)
        if relay:

            @pl.when(is_end)
            def _():
                r.far_got[3 - kv] = jnp.zeros(r.far_got.shape[1:], jnp.bfloat16)

    def guarded(condition, action):
        if condition is None:
            action()
        else:
            pl.when(condition)(action)

    def direct(j, o):
        slot = 1 if relay else o - 1
        where = buddy if relay else shifted(kv, o, n)
        return pltpu.make_async_remote_copy(
            src_ref=r.sent.at[j, where],
            dst_ref=r.got.at[j, slot],
            send_sem=r.sum_send.at[j, slot],
            recv_sem=r.sum_recv.at[j, slot],
            device_id={"kv": where, "tp": tp},
            device_id_type=MESH,
        )

    reach = (1,) if relay else tuple(range(1, n))

    vectors = [
        (r.bound_in, r.bound),
        (r.gain_in, r.gain),
        (r.gain_one_in, r.gain_one),
        (r.bias_one_in, r.bias_one),
        (r.gain_two_in, r.gain_two),
        (r.bias_two_in, r.bias_two),
    ]
    is_end = (kv == 0) | (kv == n - 1)
    is_relay = (kv != 0) & (kv != n - 1)
    lead = min(2, groups)

    def to_relay(j, i):
        return pltpu.make_async_remote_copy(
            src_ref=r.sent.at[j, 3 - (buddy if i else kv)],
            dst_ref=r.relay_got.at[j, i],
            send_sem=r.relay_send.at[j, i],
            recv_sem=r.relay_recv.at[j, i],
            device_id={"kv": buddy, "tp": tp},
            device_id_type=MESH,
        )

    def from_relay(j, i):
        target = 3 - (kv if i else buddy)
        return target, pltpu.make_async_remote_copy(
            src_ref=r.relay_sent.at[j, i],
            dst_ref=r.got.at[j, 0],
            send_sem=r.relay_send.at[j, i],
            recv_sem=r.sum_recv.at[j, 0],
            device_id={"kv": target, "tp": tp},
            device_id_type=MESH,
        )

    def project(j):
        for w in range(kinds):
            loads[j, w].wait()
            value = jnp.dot(
                r.tokens[...], r.pool[j * kinds + w], preferred_element_type=jnp.float32
            ).reshape(n, rows, wide)
            r.whole[j, w] = value
            r.sent[j, :, w] = value.astype(jnp.bfloat16)

    def send_far(j):
        if relay:

            @pl.when(is_end)
            def _():
                for i in range(2):
                    to_relay(j, i).start()

    def send_near(j, chosen):
        def start():
            for o in reach:
                direct(j, o).start()

        guarded(chosen, start)

    def pass_relay(j):
        if not relay:
            return

        @pl.when(is_relay)
        def _():
            for i in range(2):
                to_relay(j, i).wait_recv()
                target, copy = from_relay(j, i)
                for w in range(kinds):
                    total = r.whole[j, w, target] + r.relay_got[j, i, w].astype(jnp.float32)
                    r.relay_sent[j, i, w] = total.astype(jnp.bfloat16)
                copy.start()

    def finish_sends(j):
        for o in reach:
            direct(j, o).wait_send()
        if relay:
            for i in range(2):
                to_relay(j, i).wait_send()

    def load_state(j):
        part = pl.ds(j * heads, heads)
        state_loads[j] = store(r.state.at[:, part], r.new_state.at[:, part], r.load_state.at[j])

    pending = []

    def wait_sums(j):
        if relay:
            from_relay(j, 0)[1].wait_recv()
        for o in reach:
            direct(j, o).wait_recv()

    def prepare(j):
        def summed(w):
            total = r.whole[j, w, kv]
            for slot in range(r.got.shape[1]):
                total = total + r.got[j, slot, w].astype(jnp.float32)
            return total.astype(jnp.bfloat16).astype(jnp.float32)

        query_raw, forget_raw, value, gate = (summed(w) for w in range(kinds))
        low = r.bound[:, j * wide : (j + 1) * wide]
        forget = low + (1.0 - low) * jax.nn.sigmoid(forget_raw)
        query = query_raw * jax.nn.sigmoid(query_raw)
        stacked = []
        for factor in (forget, query):
            high = factor.astype(jnp.bfloat16).astype(jnp.float32)
            stacked += [high, factor - high]
        turned = jnp.concatenate(stacked, axis=0).T.reshape(heads, size, 4 * rows)
        r.factors[...] = turned.astype(jnp.bfloat16)
        for h in range(heads):
            pair = value[:, (h // 2) * lanes : (h // 2 + 1) * lanes]
            r.value[h] = pltpu.roll(pair, size, 1) if h % 2 else pair
        r.gate[...] = gate * jax.nn.sigmoid(gate)

    def update(j):
        state_loads[j].wait()

        def one_head(h, slot):
            r.spread[slot] = jnp.dot(
                r.factors[h], r.pick[...], preferred_element_type=jnp.float32
            )
            for b in range(rows):
                base = b * 2 * lanes
                line = r.value[h, b : b + 1, :size]
                keep = r.spread[slot, :, base : base + size]
                query_column = r.spread[slot, :, base + lanes : base + lanes + size]
                updated = line + keep * (r.new_state[b, j * heads + h] - line)
                r.new_state[b, j * heads + h] = updated
                r.read[h, b : b + 1] = jnp.sum(updated * query_column, axis=0, keepdims=True)

        def two_heads(i, carry):
            for slot in range(2):
                one_head(i * 2 + slot, slot)
            return carry

        lax.fori_loop(0, heads // 2, two_heads, 0)

    def gated_out(j):
        def normalized(h):
            whole = r.read[h]
            return whole * lax.rsqrt(jnp.mean(whole * whole, axis=1, keepdims=True) + epsilon)

        for p in range(heads // 2):
            here = slice(p * lanes, (p + 1) * lanes)
            pair = jnp.concatenate([normalized(2 * p), normalized(2 * p + 1)], axis=1)
            gated = pair * r.gain[...] * r.gate[:, here]
            r.gathered[j, kv, :, here] = gated.astype(jnp.bfloat16)
        for o in range(1, n):
            guarded(sends_mix(j, o), mix_copy(j, o).start)

    def mix_copy(j, o):
        return pltpu.make_async_remote_copy(
            src_ref=r.gathered.at[j, kv],
            dst_ref=r.gathered.at[j, kv],
            send_sem=r.mix_send.at[j, o],
            recv_sem=r.mix_recv.at[j, o],
            device_id=at(o, 0),
            device_id_type=MESH,
        )

    def hops(j):
        return relay and j < groups - 1

    def sends_mix(j, o):
        return (kv != 3 if o == 1 else kv != 0 if o == 3 else is_relay) if hops(j) else None

    def forward_mix(j, i):
        return pltpu.make_async_remote_copy(
            src_ref=r.gathered.at[j, buddy],
            dst_ref=r.gathered.at[j, buddy],
            send_sem=r.mix_forward.at[j, i],
            recv_sem=r.mix_recv.at[j, 5 - 2 * kv if i else 2],
            device_id={"kv": 3 - (buddy if i else kv), "tp": tp},
            device_id_type=MESH,
        )

    def forward_mixes(j):
        if not hops(j):
            return

        @pl.when(is_relay)
        def _():
            pltpu.make_async_remote_copy(
                src_ref=r.gathered.at[j, kv],
                dst_ref=r.gathered.at[j, buddy],
                send_sem=r.mix_send.at[j, 1],
                recv_sem=r.mix_recv.at[j, 2 * kv - 1],
                device_id={"kv": buddy, "tp": tp},
                device_id_type=MESH,
            ).wait_recv()
            for i in range(2):
                forward_mix(j, i).start()

    def finish_mixes(j):
        for o in range(1, n):
            guarded(sends_mix(j, o), mix_copy(j, o).wait_send)
        if hops(j):

            @pl.when(is_relay)
            def _():
                for i in range(2):
                    forward_mix(j, i).wait_send()

    def wait_mixes(j):
        for o in range(1, n):
            condition = None
            if hops(j) and o != 2:
                condition = kv != (1 if o == 1 else 2)
            guarded(condition, mix_copy(j, o).wait_recv)

    def project_out(j):
        whole = r.gathered[j].reshape(count, wide)
        for u in range(t):
            if j == 0:
                loads_out[u].wait()
            product = jnp.dot(
                whole,
                r.out_buf[u, j * wide : (j + 1) * wide],
                preferred_element_type=jnp.float32,
            )
            r.mixed[u] = product if j == 0 else r.mixed[u] + product

    loads_out, loads_up, loads_down, state_loads = {}, {}, {}, {}
    up_chunks, _, up_width = r.up_buf.shape
    dests = [shifted(kv, o, n) for o in [*range(1, n), 0]]
    if relay:
        tables = [(3, 2, 1, 0), (2, 0, 3, 1), (1, 3, 0, 2), (0, 1, 2, 3)]
        dests = [
            jnp.where(kv < 2, jnp.where(kv == 0, a, b), jnp.where(kv == 2, c, d))
            for a, b, c, d in zip(*tables)
        ]

    def load_rest():
        for u in range(t):
            loads_out[u] = store(
                r.w_out.at[:, columns_of(shifted(tp, u, t))], r.out_buf.at[u], r.load_out.at[u]
            )
        for c in range(up_chunks):
            loads_up[c] = store(
                r.w_up.at[:, pl.ds(c * up_width, up_width)], r.up_buf.at[c], r.load_up.at[c]
            )
        for s in range(n):
            for u in [*range(1, t), 0]:
                for p in range(pieces):
                    slot = (s * t + u) * pieces + p
                    part = pl.ds(p * depth_down, depth_down)
                    loads_down[s, u, p] = store(
                        r.w_down.at[part, columns_of(dests[s] * t + shifted(tp, u, t))],
                        r.down.at[slot],
                        r.load_down.at[slot],
                    )

    affines = []

    def send_affine():
        for copy in small[1:]:
            copy.wait()
        r.affine[me, 0:1] = r.gain_one[...]
        r.affine[me, 1:2] = r.bias_one[...]
        for o, u in offsets:
            affines.append(
                send(
                    r.affine.at[me],
                    r.affine.at[me],
                    r.affine_send.at[o, u],
                    r.affine_recv.at[o, u],
                    at(o, u),
                )
            )
        pending.extend(affines)

    def pair_sum():
        parts = []
        for u in range(1, t):
            parts.append(
                send(
                    r.mixed.at[u],
                    r.part_got.at[u - 1],
                    r.part_send.at[u],
                    r.part_recv.at[u],
                    at(0, u),
                )
            )
        pending.extend(parts)
        own_tokens = r.tokens[:, columns_of(tp)].astype(jnp.float32)
        first = residual_scale * own_tokens + r.mixed[0]
        for u in range(1, t):
            parts[u - 1].wait_recv()
            first = first + r.part_got[u - 1]
        r.mixed[0] = first
        r.firsts[me] = first.astype(jnp.bfloat16)

    def hand_over(index, o, u, where):
        return pltpu.make_async_remote_copy(
            src_ref=r.firsts.at[index],
            dst_ref=r.firsts.at[index],
            send_sem=r.first_send.at[o, u],
            recv_sem=r.first_recv.at[o, u],
            device_id=where,
            device_id_type=MESH,
        )

    def tell_first():
        first = r.mixed[0]
        total = jnp.sum(first, axis=1, keepdims=True)
        away = first - total / columns
        r.tallies[0, 0:2] = jnp.concatenate(
            [to_lanes(total), to_lanes(jnp.sum(away * away, axis=1, keepdims=True))], axis=0
        )
        for i, (o, u) in enumerate(offsets):
            counts.append(
                send(
                    r.tallies.at[0],
                    r.tallies.at[i + 1],
                    r.tally_send.at[i],
                    r.tally_recv.at[i],
                    at(o, u),
                )
            )
        pending.extend(counts)

    counts = []
    def straight(o):
        return (kv != 0 if o == 3 else kv != 3) if relay and o != 2 else None

    def send_firsts():
        for u in range(1, t):
            copy = hand_over(me, 0, u, at(0, u))
            copy.start()
            pending.append(copy)
        for o in sorted(range(1, n), key=lambda o: -min(o, n - o)):
            copy = hand_over(me, o, 0, at(o, 0))
            guarded(straight(o), copy.start)

    def forward_first():
        return pltpu.make_async_remote_copy(
            src_ref=r.firsts.at[block(2, 0)],
            dst_ref=r.firsts.at[block(2, 0)],
            send_sem=r.forward_send,
            recv_sem=r.first_recv.at[2 * kv - 1, 0],
            device_id={"kv": buddy, "tp": tp},
            device_id_type=MESH,
        )

    def finish_firsts():
        for o in range(1, n):
            guarded(straight(o), hand_over(me, o, 0, at(o, 0)).wait_send)
        if relay:
            pl.when(is_relay)(lambda: forward_first().wait_send())

    def first_stats():
        for copy in affines:
            copy.wait_recv()
        for copy in counts:
            copy.wait_recv()
        tallies = [r.tallies[i, 0:2] for i in range(group)]
        center = sum(tally[0:1] for tally in tallies) / width
        spread = jnp.zeros_like(center)
        for tally in tallies:
            away = tally[0:1] / columns - center
            spread = spread + tally[1:2] + columns * (away * away)
        scale = lax.rsqrt(spread / width + epsilon)
        r.center[...] = jnp.broadcast_to(to_sublanes(center), r.center.shape)
        r.scale[...] = jnp.broadcast_to(to_sublanes(scale), r.scale.shape)

    def wait_first(o, u):
        hand_over(block(n - o, 0), o, u, at(0, u)).wait_recv()
        if u == 0:
            for v in range(1, t):
                copy = hand_over(block(n - o, 0), o, v, at(0, v))
                copy.start()
                pending.append(copy)

    def forward():
        if relay:
            pl.when(is_relay)(lambda: forward_first().start())

    def go_up(o, u, first_one):
        index = block(n - o, t - u)
        pair = r.affine[index]
        center, scale = r.center[:, 0:1], r.scale[:, 0:1]
        away = r.firsts[index].astype(jnp.float32) - center
        normed = (away * scale * pair[0:1] + pair[1:2]).astype(jnp.bfloat16)
        if first_one:
            r.own_normed[...] = normed
        for c in range(up_chunks):
            here = slice(c * up_width, (c + 1) * up_width)
            if first_one:
                loads_up[c].wait()
            product = jnp.dot(
                normed, r.up_buf[c, columns_of(index)], preferred_element_type=jnp.float32
            )
            r.upper[:, here] = product if first_one else r.upper[:, here] + product

    def square():
        upper = jnp.maximum(r.upper[...], 0.0)
        r.hidden[...] = (upper * upper).astype(jnp.bfloat16)

    near = {}

    def go_down(s, u):
        product = jnp.zeros((count, columns), jnp.float32)
        for p in range(pieces):
            loads_down[s, u, p].wait()
            product = product + jnp.dot(
                r.hidden[:, p * depth_down : (p + 1) * depth_down],
                r.down[(s * t + u) * pieces + p],
                preferred_element_type=jnp.float32,
            )
        if u:
            r.near_sent[s, u - 1] = product.astype(jnp.bfloat16)
            near[s, u] = send(
                r.near_sent.at[s, u - 1],
                r.near_got.at[s, u - 1],
                r.near_send.at[s, u - 1],
                r.near_recv.at[s, u - 1],
                at(0, u),
            )
        else:
            r.kept[s] = product

    def near_sum(s):
        value = r.kept[s]
        for u in range(1, t):
            near[s, u].wait_recv()
            value = value + r.near_got[s, u - 1].astype(jnp.float32)
        return value

    def far_copy(s, where):
        return pltpu.make_async_remote_copy(
            src_ref=r.far_sent.at[s],
            dst_ref=r.far_got.at[kv],
            send_sem=r.far_send.at[s],
            recv_sem=r.far_recv.at[kv],
            device_id={"kv": where, "tp": tp},
            device_id_type=MESH,
        )

    def far_relay():
        return pltpu.make_async_remote_copy(
            src_ref=r.far_sent.at[0],
            dst_ref=r.far_relay,
            send_sem=r.far_send.at[0],
            recv_sem=r.far_relay_recv,
            device_id={"kv": buddy, "tp": tp},
            device_id_type=MESH,
        )

    def far_out(s):
        value = near_sum(s)
        if relay and s == 0:
            r.far_sent[s] = value.astype(jnp.bfloat16)
            pl.when(is_end)(lambda: far_relay().start())
            pl.when(is_relay)(lambda: far_copy(s, dests[s]).start())
        elif relay and s == 2:
            r.kept[s] = value

            @pl.when(is_relay)
            def _():
                far_relay().wait_recv()
                r.kept[s] = r.kept[s] + r.far_relay[...].astype(jnp.float32)

            r.far_sent[s] = r.kept[s].astype(jnp.bfloat16)
            far_copy(s, dests[s]).start()
        else:
            r.far_sent[s] = value.astype(jnp.bfloat16)
            far_copy(s, dests[s]).start()

    def far_arrival(o):
        sender = shifted(kv, o, n)
        return pltpu.make_async_remote_copy(
            src_ref=r.far_sent.at[0],
            dst_ref=r.far_got.at[sender],
            send_sem=r.far_send.at[0],
            recv_sem=r.far_recv.at[sender],
            device_id={"kv": sender, "tp": tp},
            device_id_type=MESH,
        )

    def second_sum():
        second = residual_scale * r.own_normed[...].astype(jnp.float32) + near_sum(n - 1)
        for o in range(1, n):
            guarded(straight(o), far_arrival(o).wait_recv)
            second = second + r.far_got[shifted(kv, o, n)].astype(jnp.float32)
        r.kept[0] = second
        pending.extend(near.values())

    def second_norm():
        second = r.kept[0]
        sums = jnp.concatenate(
            [
                to_lanes(jnp.sum(second, axis=1, keepdims=True)),
                to_lanes(jnp.sum(second * second, axis=1, keepdims=True)),
            ],
            axis=0,
        )
        r.stats[0, 0:2] = sums
        tallies = []
        for i, (o, u) in enumerate(offsets):
            tallies.append(
                send(
                    r.stats.at[0],
                    r.stats.at[i + 1],
                    r.stats_send.at[i],
                    r.stats_recv.at[i],
                    at(o, u),
                )
            )
        pending.extend(tallies)
        for i, copy in enumerate(tallies):
            copy.wait_recv()
            sums = sums + r.stats[i + 1, 0:2]
        center_two = to_sublanes(sums[0:1]) / width
        spread_two = to_sublanes(sums[1:2]) / width - center_two * center_two
        result = (second - center_two) * lax.rsqrt(spread_two + epsilon)
        r.out[...] = (result * r.gain_two[...] + r.bias_two[...]).astype(jnp.bfloat16)

    def drain():
        for j in range(groups):
            finish_sends(j)
            finish_mixes(j)
        finish_firsts()
        for s in range(n - 1):
            far_copy(s, dests[s]).wait_send()
        for copy in pending:
            copy.wait_send()

    load_small([(r.tokens_in, r.tokens)])
    load_weights(0)
    greet_all()
    for j in range(1, groups):
        load_weights(j)
    load_small(vectors)
    wait_tokens()
    for j in range(groups):
        project(j)
        if j == 0:
            wait_barrier()
        send_far(j)
        send_near(j, is_relay if relay else None)
        if relay and j:
            send_near(j - 1, is_end)
        load_state(j)
    if relay:
        send_near(groups - 1, is_end)
    load_rest()
    for j in range(lead):
        pass_relay(j)
    send_affine()
    fill()
    for j in range(groups):
        wait_sums(j)
        prepare(j)
        update(j)
        gated_out(j)
        if j + lead < groups:
            pass_relay(j + lead)
    for j in range(groups):
        forward_mixes(j)
    for j in range(groups):
        wait_mixes(j)
        project_out(j)
    pair_sum()
    tell_first()
    send_firsts()
    wait_first(arrivals[0], 0)
    forward()
    first_stats()
    go_up(0, 0, True)
    for u in range(1, t):
        wait_first(0, u)
        go_up(0, u, False)
    for i in range(n - 1):
        if i:
            wait_first(arrivals[i], 0)
        go_up(arrivals[i], 0, False)
        if i:
            for u in range(1, t):
                wait_first(arrivals[i - 1], u)
                go_up(arrivals[i - 1], u, False)
    for u in range(1, t):
        wait_first(arrivals[-1], u)
        go_up(arrivals[-1], u, False)
    square()
    for s in range(n):
        for u in range(1, t):
            go_down(s, u)
        if s:
            far_out(s - 1)
        go_down(s, 0)
    second_sum()
    second_norm()
    drain()


def layer(n, t, tokens, state, weights, bound, gain, w_out, w_up, w_down, affine):
    count, depth = tokens.shape
    rows = count // n
    width = weights[0].shape[1]
    kinds = len(weights)
    size = state.shape[3]
    lanes = 2 * size
    wide = min(width, 8 * size)
    groups = width // wide
    heads = wide // size
    columns = affine[0].shape[1]
    model, units = w_up.shape
    group = n * t
    up_width = min(units, 512)
    dma = pltpu.SemaphoreType.DMA
    vmem = pltpu.VMEM
    few, many = jnp.bfloat16, jnp.float32
    shares = columns == wide and units % depth == 0 and group * (units // depth) == groups * kinds
    pieces = units // depth if shares else 1
    inputs = {
        "tokens_in": tokens,
        "state": state,
        "w_query": weights[0],
        "w_forget": weights[1],
        "w_input": weights[2],
        "w_gate": weights[3],
        "bound_in": bound,
        "gain_in": gain,
        "w_out": w_out,
        "w_up": w_up,
        "w_down": w_down,
        "gain_one_in": affine[0],
        "bias_one_in": affine[1],
        "gain_two_in": affine[2],
        "bias_two_in": affine[3],
    }
    scratch = {
        "tokens": vmem(tokens.shape, few),
        "bound": vmem(bound.shape, many),
        "gain": vmem(gain.shape, many),
        "gain_one": vmem((1, columns), many),
        "bias_one": vmem((1, columns), many),
        "gain_two": vmem((1, columns), many),
        "bias_two": vmem((1, columns), many),
        "pool": vmem((groups * kinds, depth, wide), few),
        "whole": vmem((groups, kinds, n, rows, wide), many),
        "sent": vmem((groups, n, kinds, rows, wide), few),
        "got": vmem((groups, 2 if n == 4 else n - 1, kinds, rows, wide), few),
        "relay_got": vmem((groups, 2, kinds, rows, wide), few),
        "relay_sent": vmem((groups, 2, kinds, rows, wide), few),
        "pick": vmem((4 * rows, rows * 2 * lanes), few),
        "factors": vmem((heads, size, 4 * rows), few),
        "value": vmem((heads, rows, lanes), many),
        "gate": vmem((rows, wide), many),
        "spread": vmem((2, size, rows * 2 * lanes), many),
        "read": vmem((heads, rows, size), many),
        "gathered": vmem((groups, n, rows, wide), few),
        "out_buf": vmem((t, width, columns), few),
        "mixed": vmem((t, count, columns), many),
        "up_buf": vmem((units // up_width, model, up_width), few),
        "part_got": vmem((t - 1, count, columns), many),
        "affine": vmem((group, 2, columns), many),
        "firsts": vmem((group, count, columns), few),
        "tallies": vmem((group, 8, count), many),
        "center": vmem((count, 128), many),
        "scale": vmem((count, 128), many),
        "upper": vmem((count, units), many),
        "own_normed": vmem((count, columns), few),
        "hidden": vmem((count, units), few),
        "near_sent": vmem((n, t - 1, count, columns), few),
        "near_got": vmem((n, t - 1, count, columns), few),
        "kept": vmem((n, count, columns), many),
        "far_sent": vmem((n, count, columns), few),
        "far_got": vmem((n, count, columns), few),
        "far_relay": vmem((count, columns), few),
        "stats": vmem((group, 8, count), many),
        "small_sem": dma((7,)),
        "load_project": dma((groups * kinds,)),
        "load_state": dma((groups,)),
        "load_out": dma((t,)),
        "load_up": dma((units // up_width,)),
        "load_down": dma((group * pieces,)),
        "sum_send": dma((groups, n - 1)),
        "sum_recv": dma((groups, n - 1)),
        "relay_send": dma((groups, 2)),
        "relay_recv": dma((groups, 2)),
        "forward_send": dma,
        "far_relay_recv": dma,
        "mix_send": dma((groups, n)),
        "mix_recv": dma((groups, n)),
        "mix_forward": dma((groups, 2)),
        "tally_send": dma((group,)),
        "tally_recv": dma((group,)),
        "part_send": dma((t,)),
        "part_recv": dma((t,)),
        "affine_send": dma((n, t)),
        "affine_recv": dma((n, t)),
        "first_send": dma((n, t)),
        "first_recv": dma((n, t)),
        "near_send": dma((n, t)),
        "near_recv": dma((n, t)),
        "far_send": dma((n,)),
        "far_recv": dma((n,)),
        "stats_send": dma((group,)),
        "stats_recv": dma((group,)),
    }
    if not shares:
        scratch["down"] = vmem((group, units, columns), few)

    def kernel(*refs):
        names = [*inputs, "out", "new_state", *scratch]
        if shares:
            names.append("down")
            refs = (*refs, refs[names.index("pool")])
        layer_kernel(n, t, size, names, *refs)

    return pl.pallas_call(
        kernel,
        out_shape=(vmem((count, columns), few), vmem(state.shape, many)),
        in_specs=[pl.BlockSpec(memory_space=pl.ANY)] * len(inputs),
        out_specs=(pl.BlockSpec(memory_space=pltpu.VMEM),) * 2,
        scratch_shapes=list(scratch.values()),
        compiler_params=pltpu.CompilerParams(
            collective_id=0, has_side_effects=True, vmem_limit_bytes=LAYER_BYTES
        ),
        name="layer",
    )(*inputs.values())


def write_kernel(result, new_state, result_out, state_out, sem):
    pieces = sem.shape[0] - 1
    heads = new_state.shape[1] // pieces
    copies = [store(result, result_out, sem.at[pieces])]
    for i in range(pieces):
        part = pl.ds(i * heads, heads)
        copies.append(store(new_state.at[:, part], state_out.at[:, part], sem.at[i]))
    for copy in copies:
        copy.wait()


def write_out(result, new_state):
    return pl.pallas_call(
        write_kernel,
        out_shape=(
            jax.ShapeDtypeStruct(result.shape, result.dtype),
            jax.ShapeDtypeStruct(new_state.shape, new_state.dtype),
        ),
        in_specs=[pl.BlockSpec(memory_space=pltpu.VMEM)] * 2,
        out_specs=(pl.BlockSpec(memory_space=pl.ANY),) * 2,
        scratch_shapes=[pltpu.SemaphoreType.DMA((9,))],
        compiler_params=pltpu.CompilerParams(vmem_limit_bytes=WRITE_BYTES),
        name="write",
    )(result, new_state)


def per_device(
    tokens,
    state,
    w_query,
    w_forget,
    w_input,
    w_gate,
    lower_bound,
    head_gain,
    w_out,
    gain_one,
    bias_one,
    w_up,
    w_down,
    gain_two,
    bias_two,
):
    n, t = lax.axis_size("kv"), lax.axis_size("tp")
    result, new_state = layer(
        n,
        t,
        tokens,
        state,
        (w_query, w_forget, w_input, w_gate),
        lower_bound[None, :],
        jnp.tile(head_gain, 2)[None, :],
        w_out,
        w_up,
        w_down,
        [vector[None, :] for vector in (gain_one, bias_one, gain_two, bias_two)],
    )
    return write_out(result, new_state)


def solution(mesh):
    placed = (
        P("dp", "kv"),
        P(("dp", "kv"), "tp", None, None),
        P("kv", "tp"),
        P("kv", "tp"),
        P("kv", "tp"),
        P("kv", "tp"),
        P("tp"),
        P(),
        P("tp", "kv"),
        P(("kv", "tp")),
        P(("kv", "tp")),
        P(None, ("kv", "tp")),
        P(("kv", "tp"), None),
        P(("kv", "tp")),
        P(("kv", "tp")),
    )
    return jax.shard_map(
        per_device,
        mesh=mesh,
        in_specs=placed,
        out_specs=(P("dp", ("kv", "tp")), P(("dp", "kv"), "tp", None, None)),
        check_vma=False,
    )
```

```python
import functools
import types

import jax
import jax.numpy as jnp
import numpy as np
from jax import lax
from jax.experimental import pallas as pl
from jax.experimental.pallas import tpu as pltpu
from jax.sharding import PartitionSpec as P

epsilon = 0.1
residual_scale = 1.68
MESH = pl.DeviceIdType.MESH
LAYER_BYTES = 47 * 1024 * 1024
WRITE_BYTES = 1024 * 1024
GROUP_HEADS = 4
LAG = 3
LEAD = 5


def shifted(index, by, count):
    return lax.rem(index + by, count)


def greet(peers):
    barrier = pltpu.get_barrier_semaphore()
    for peer in peers:
        pl.semaphore_signal(barrier, inc=1, device_id=peer, device_id_type=MESH)
    return lambda: pl.semaphore_wait(barrier, len(peers))


def send(source, target, send_sem, recv_sem, peer):
    copy = pltpu.make_async_remote_copy(
        src_ref=source,
        dst_ref=target,
        send_sem=send_sem,
        recv_sem=recv_sem,
        device_id=peer,
        device_id_type=MESH,
    )
    copy.start()
    return copy


def store(source, target, sem):
    copy = pltpu.make_async_copy(source, target, sem)
    copy.start()
    return copy


def to_lanes(column):
    count = column.shape[0]
    diagonal = lax.broadcasted_iota(jnp.int32, (count, count), 0) == lax.broadcasted_iota(
        jnp.int32, (count, count), 1
    )
    return jnp.sum(jnp.where(diagonal, column, 0.0), axis=0, keepdims=True)


def to_sublanes(row):
    count = row.shape[1]
    diagonal = lax.broadcasted_iota(jnp.int32, (count, count), 0) == lax.broadcasted_iota(
        jnp.int32, (count, count), 1
    )
    return jnp.sum(jnp.where(diagonal, row, 0.0), axis=1, keepdims=True)


def fill_pick(pick, rows, lanes):
    shape = (4 * rows, 2 * lanes)
    line = lax.broadcasted_iota(jnp.int32, shape, 0)
    lane = lax.broadcasted_iota(jnp.int32, shape, 1)
    same_half = (line < 2 * rows) == (lane < lanes)
    row = lax.rem(line, rows)
    for b in range(rows):
        chosen = jnp.where(same_half & (row == b), 1.0, 0.0)
        pick[:, b * 2 * lanes : (b + 1) * 2 * lanes] = chosen.astype(jnp.bfloat16)


def layer_kernel(n, t, size, names, *refs):
    r = types.SimpleNamespace(**dict(zip(names, refs)))
    kv, tp = lax.axis_index("kv"), lax.axis_index("tp")
    count, columns = r.out.shape
    rows = count // n
    group = n * t
    me = kv * t + tp
    width = group * columns
    groups, kinds, _, _, wide = r.whole.shape
    heads = wide // size
    lanes = 2 * size
    pieces = r.down.shape[0] // group
    depth_down = r.down.shape[1]
    offsets = [(o, u) for o in range(n) for u in range(t) if (o, u) != (0, 0)]
    relay = n == 4
    buddy = kv + 1 - 2 * lax.rem(kv, 2)

    def at(o, u):
        return {"kv": shifted(kv, o, n), "tp": shifted(tp, u, t)}

    def block(o, u):
        return shifted(kv, o, n) * t + shifted(tp, u, t)

    arrivals = sorted(range(1, n), key=lambda o: min(o, n - o))
    if relay:
        arrivals = [2, 3 - 2 * (kv // 2), 1 + 2 * (kv // 2)]

    def columns_of(index):
        return pl.ds(pl.multiple_of(index * columns, columns), columns)

    barrier = pltpu.get_barrier_semaphore()

    def greet_all():
        for o, u in offsets:
            pl.semaphore_signal(barrier, inc=1, device_id=at(o, u), device_id_type=MESH)

    def wait_barrier():
        pl.semaphore_wait(barrier, len(offsets))

    small = []

    def load_small(pairs):
        for source, target in pairs:
            small.append(store(source, target, r.small_sem.at[len(small)]))

    weights = (r.w_query, r.w_forget, r.w_input, r.w_gate)
    loads = {}

    span = r.pool.shape[2]
    parts = span // wide

    def load_weights(c):
        for w in range(kinds):
            loads[c, w] = store(
                weights[w].at[:, pl.ds(c * span, span)],
                r.pool.at[c * kinds + w],
                r.load_project.at[c * kinds + w],
            )

    def wait_tokens():
        small[0].wait()

    def fill():
        fill_pick(r.pick, rows, lanes)
        if relay:

            @pl.when(is_end)
            def _():
                r.far_got[3 - kv] = jnp.zeros(r.far_got.shape[1:], jnp.bfloat16)

    def guarded(condition, action):
        if condition is None:
            action()
        else:
            pl.when(condition)(action)

    def direct(j, o):
        slot = 1 if relay else o - 1
        where = buddy if relay else shifted(kv, o, n)
        return pltpu.make_async_remote_copy(
            src_ref=r.sent.at[j, where],
            dst_ref=r.got.at[j, slot],
            send_sem=r.sum_send.at[j, slot],
            recv_sem=r.sum_recv.at[j, slot],
            device_id={"kv": where, "tp": tp},
            device_id_type=MESH,
        )

    reach = (1,) if relay else tuple(range(1, n))

    vectors = [
        (r.bound_in, r.bound),
        (r.gain_in, r.gain),
        (r.gain_one_in, r.gain_one),
        (r.bias_one_in, r.bias_one),
        (r.gain_two_in, r.gain_two),
        (r.bias_two_in, r.bias_two),
    ]
    is_end = (kv == 0) | (kv == n - 1)
    is_relay = (kv != 0) & (kv != n - 1)
    lag = LAG
    lead = min(LEAD, groups)

    def to_relay(j, i):
        return pltpu.make_async_remote_copy(
            src_ref=r.sent.at[j, 3 - (buddy if i else kv)],
            dst_ref=r.relay_got.at[j, i],
            send_sem=r.relay_send.at[j, i],
            recv_sem=r.relay_recv.at[j, i],
            device_id={"kv": buddy, "tp": tp},
            device_id_type=MESH,
        )

    def from_relay(j, i):
        target = 3 - (kv if i else buddy)
        return target, pltpu.make_async_remote_copy(
            src_ref=r.relay_sent.at[j, i],
            dst_ref=r.got.at[j, 0],
            send_sem=r.relay_send.at[j, i],
            recv_sem=r.sum_recv.at[j, 0],
            device_id={"kv": target, "tp": tp},
            device_id_type=MESH,
        )

    def project(c):
        for w in range(kinds):
            loads[c, w].wait()
            value = jnp.dot(
                r.tokens[...], r.pool[c * kinds + w], preferred_element_type=jnp.float32
            ).reshape(n, rows, span)
            for p in range(parts):
                here = value[:, :, p * wide : (p + 1) * wide]
                r.whole[c * parts + p, w] = here
                r.sent[c * parts + p, :, w] = here.astype(jnp.bfloat16)

    def send_far(j):
        if relay:

            @pl.when(is_end)
            def _():
                for i in range(2):
                    to_relay(j, i).start()

    def send_near(j, chosen):
        def start():
            for o in reach:
                direct(j, o).start()

        guarded(chosen, start)

    def pass_relay(j):
        if not relay:
            return

        @pl.when(is_relay)
        def _():
            for i in range(2):
                to_relay(j, i).wait_recv()
                target, copy = from_relay(j, i)
                for w in range(kinds):
                    total = r.whole[j, w, target] + r.relay_got[j, i, w].astype(jnp.float32)
                    r.relay_sent[j, i, w] = total.astype(jnp.bfloat16)
                copy.start()

    def finish_sends(j):
        for o in reach:
            direct(j, o).wait_send()
        if relay:
            for i in range(2):
                to_relay(j, i).wait_send()

    def load_state(j):
        part = pl.ds(j * heads, heads)
        state_loads[j] = store(r.state.at[:, part], r.new_state.at[:, part], r.load_state.at[j])

    pending = []

    def wait_sums(j):
        if relay:
            from_relay(j, 0)[1].wait_recv()
        for o in reach:
            direct(j, o).wait_recv()

    def prepare(j):
        def summed(w):
            total = r.whole[j, w, kv]
            for slot in range(r.got.shape[1]):
                total = total + r.got[j, slot, w].astype(jnp.float32)
            return total.astype(jnp.bfloat16).astype(jnp.float32)

        query_raw, forget_raw, value, gate = (summed(w) for w in range(kinds))
        low = r.bound[:, j * wide : (j + 1) * wide]
        forget = low + (1.0 - low) * jax.nn.sigmoid(forget_raw)
        query = query_raw * jax.nn.sigmoid(query_raw)
        stacked = []
        for factor in (forget, query):
            high = factor.astype(jnp.bfloat16).astype(jnp.float32)
            stacked += [high, factor - high]
        turned = jnp.concatenate(stacked, axis=0).T.reshape(heads, size, 4 * rows)
        r.factors[...] = turned.astype(jnp.bfloat16)
        for h in range(heads):
            pair = value[:, (h // 2) * lanes : (h // 2 + 1) * lanes]
            r.value[h] = pltpu.roll(pair, size, 1) if h % 2 else pair
        r.gate[...] = gate * jax.nn.sigmoid(gate)

    def update(j):
        state_loads[j].wait()

        def one_head(h, slot):
            r.spread[slot] = jnp.dot(
                r.factors[h], r.pick[...], preferred_element_type=jnp.float32
            )
            for b in range(rows):
                base = b * 2 * lanes
                line = r.value[h, b : b + 1, :size]
                keep = r.spread[slot, :, base : base + size]
                query_column = r.spread[slot, :, base + lanes : base + lanes + size]
                updated = line + keep * (r.new_state[b, j * heads + h] - line)
                r.new_state[b, j * heads + h] = updated
                r.read[h, b : b + 1] = jnp.sum(updated * query_column, axis=0, keepdims=True)

        def two_heads(i, carry):
            for slot in range(2):
                one_head(i * 2 + slot, slot)
            return carry

        lax.fori_loop(0, heads // 2, two_heads, 0)

    def gated_out(j):
        def normalized(h):
            whole = r.read[h]
            return whole * lax.rsqrt(jnp.mean(whole * whole, axis=1, keepdims=True) + epsilon)

        gain = jnp.concatenate([r.gain[...]] * 2, axis=1)
        for p in range(heads // 2):
            here = slice(p * lanes, (p + 1) * lanes)
            pair = jnp.concatenate([normalized(2 * p), normalized(2 * p + 1)], axis=1)
            gated = pair * gain * r.gate[:, here]
            r.gathered[j, kv, :, here] = gated.astype(jnp.bfloat16)
        for o in range(1, n):
            guarded(sends_mix(j, o), mix_copy(j, o).start)

    def mix_copy(j, o):
        return pltpu.make_async_remote_copy(
            src_ref=r.gathered.at[j, kv],
            dst_ref=r.gathered.at[j, kv],
            send_sem=r.mix_send.at[j, o],
            recv_sem=r.mix_recv.at[j, o],
            device_id=at(o, 0),
            device_id_type=MESH,
        )

    def hops(j):
        return relay and j < groups - 1

    def sends_mix(j, o):
        return (kv != 3 if o == 1 else kv != 0 if o == 3 else is_relay) if hops(j) else None

    def forward_mix(j, i):
        return pltpu.make_async_remote_copy(
            src_ref=r.gathered.at[j, buddy],
            dst_ref=r.gathered.at[j, buddy],
            send_sem=r.mix_forward.at[j, i],
            recv_sem=r.mix_recv.at[j, 5 - 2 * kv if i else 2],
            device_id={"kv": 3 - (buddy if i else kv), "tp": tp},
            device_id_type=MESH,
        )

    def forward_mixes(j):
        if not hops(j):
            return

        @pl.when(is_relay)
        def _():
            pltpu.make_async_remote_copy(
                src_ref=r.gathered.at[j, kv],
                dst_ref=r.gathered.at[j, buddy],
                send_sem=r.mix_send.at[j, 1],
                recv_sem=r.mix_recv.at[j, 2 * kv - 1],
                device_id={"kv": buddy, "tp": tp},
                device_id_type=MESH,
            ).wait_recv()
            for i in range(2):
                forward_mix(j, i).start()

    def finish_mixes(j):
        for o in range(1, n):
            guarded(sends_mix(j, o), mix_copy(j, o).wait_send)
        if hops(j):

            @pl.when(is_relay)
            def _():
                for i in range(2):
                    forward_mix(j, i).wait_send()

    def wait_mixes(j):
        for o in range(1, n):
            condition = None
            if hops(j) and o != 2:
                condition = kv != (1 if o == 1 else 2)
            guarded(condition, mix_copy(j, o).wait_recv)

    def project_out(j):
        whole = r.gathered[j].reshape(count, wide)
        for u in range(t):
            if j == 0:
                loads_out[u].wait()
            product = jnp.dot(
                whole,
                r.out_buf[u, j * wide : (j + 1) * wide],
                preferred_element_type=jnp.float32,
            )
            r.mixed[u] = product if j == 0 else r.mixed[u] + product

    loads_out, loads_up, loads_down, state_loads = {}, {}, {}, {}
    up_chunks, _, up_width = r.up_buf.shape
    dests = [shifted(kv, o, n) for o in [*range(1, n), 0]]
    if relay:
        tables = [(3, 2, 1, 0), (2, 0, 3, 1), (1, 3, 0, 2), (0, 1, 2, 3)]
        dests = [
            jnp.where(kv < 2, jnp.where(kv == 0, a, b), jnp.where(kv == 2, c, d))
            for a, b, c, d in zip(*tables)
        ]

    def load_rest():
        for u in range(t):
            loads_out[u] = store(
                r.w_out.at[:, columns_of(shifted(tp, u, t))], r.out_buf.at[u], r.load_out.at[u]
            )
        for c in range(up_chunks):
            loads_up[c] = store(
                r.w_up.at[:, pl.ds(c * up_width, up_width)], r.up_buf.at[c], r.load_up.at[c]
            )
        for s in range(n):
            for u in [*range(1, t), 0]:
                for p in range(pieces):
                    slot = (s * t + u) * pieces + p
                    part = pl.ds(p * depth_down, depth_down)
                    loads_down[s, u, p] = store(
                        r.w_down.at[part, columns_of(dests[s] * t + shifted(tp, u, t))],
                        r.down.at[slot],
                        r.load_down.at[slot],
                    )

    affines = []

    def send_affine():
        for copy in small[1:]:
            copy.wait()
        r.affine[me, 0:1] = r.gain_one[...]
        r.affine[me, 1:2] = r.bias_one[...]
        for o, u in offsets:
            affines.append(
                send(
                    r.affine.at[me],
                    r.affine.at[me],
                    r.affine_send.at[o, u],
                    r.affine_recv.at[o, u],
                    at(o, u),
                )
            )
        pending.extend(affines)

    def pair_sum():
        parts = []
        for u in range(1, t):
            parts.append(
                send(
                    r.mixed.at[u],
                    r.part_got.at[u - 1],
                    r.part_send.at[u],
                    r.part_recv.at[u],
                    at(0, u),
                )
            )
        pending.extend(parts)
        own_tokens = r.tokens[:, columns_of(tp)].astype(jnp.float32)
        first = residual_scale * own_tokens + r.mixed[0]
        for u in range(1, t):
            parts[u - 1].wait_recv()
            first = first + r.part_got[u - 1]
        r.mixed[0] = first
        r.firsts[me] = first.astype(jnp.bfloat16)

    def hand_over(index, o, u, where):
        return pltpu.make_async_remote_copy(
            src_ref=r.firsts.at[index],
            dst_ref=r.firsts.at[index],
            send_sem=r.first_send.at[o, u],
            recv_sem=r.first_recv.at[o, u],
            device_id=where,
            device_id_type=MESH,
        )

    def tell_first():
        first = r.mixed[0]
        total = jnp.sum(first, axis=1, keepdims=True)
        away = first - total / columns
        r.tallies[0, 0:2] = jnp.concatenate(
            [to_lanes(total), to_lanes(jnp.sum(away * away, axis=1, keepdims=True))], axis=0
        )
        for i, (o, u) in enumerate(offsets):
            counts.append(
                send(
                    r.tallies.at[0],
                    r.tallies.at[i + 1],
                    r.tally_send.at[i],
                    r.tally_recv.at[i],
                    at(o, u),
                )
            )
        pending.extend(counts)

    counts = []
    def straight(o):
        return (kv != 0 if o == 3 else kv != 3) if relay and o != 2 else None

    def send_firsts():
        for u in range(1, t):
            copy = hand_over(me, 0, u, at(0, u))
            copy.start()
            pending.append(copy)
        for o in sorted(range(1, n), key=lambda o: -min(o, n - o)):
            copy = hand_over(me, o, 0, at(o, 0))
            guarded(straight(o), copy.start)

    def forward_first():
        return pltpu.make_async_remote_copy(
            src_ref=r.firsts.at[block(2, 0)],
            dst_ref=r.firsts.at[block(2, 0)],
            send_sem=r.forward_send,
            recv_sem=r.first_recv.at[2 * kv - 1, 0],
            device_id={"kv": buddy, "tp": tp},
            device_id_type=MESH,
        )

    def finish_firsts():
        for o in range(1, n):
            guarded(straight(o), hand_over(me, o, 0, at(o, 0)).wait_send)
        if relay:
            pl.when(is_relay)(lambda: forward_first().wait_send())

    def first_stats():
        for copy in affines:
            copy.wait_recv()
        for copy in counts:
            copy.wait_recv()
        tallies = [r.tallies[i, 0:2] for i in range(group)]
        center = sum(tally[0:1] for tally in tallies) / width
        spread = jnp.zeros_like(center)
        for tally in tallies:
            away = tally[0:1] / columns - center
            spread = spread + tally[1:2] + columns * (away * away)
        scale = lax.rsqrt(spread / width + epsilon)
        r.center[...] = jnp.broadcast_to(to_sublanes(center), r.center.shape)
        r.scale[...] = jnp.broadcast_to(to_sublanes(scale), r.scale.shape)

    def wait_first(o, u):
        hand_over(block(n - o, 0), o, u, at(0, u)).wait_recv()
        if u == 0:
            for v in range(1, t):
                copy = hand_over(block(n - o, 0), o, v, at(0, v))
                copy.start()
                pending.append(copy)

    def forward():
        if relay:
            pl.when(is_relay)(lambda: forward_first().start())

    def go_up(o, u, first_one):
        index = block(n - o, t - u)
        pair = r.affine[index]
        center, scale = r.center[:, 0:1], r.scale[:, 0:1]
        away = r.firsts[index].astype(jnp.float32) - center
        normed = (away * scale * pair[0:1] + pair[1:2]).astype(jnp.bfloat16)
        if first_one:
            r.own_normed[...] = normed
        for c in range(up_chunks):
            here = slice(c * up_width, (c + 1) * up_width)
            if first_one:
                loads_up[c].wait()
            product = jnp.dot(
                normed, r.up_buf[c, columns_of(index)], preferred_element_type=jnp.float32
            )
            r.upper[:, here] = product if first_one else r.upper[:, here] + product

    def square():
        upper = jnp.maximum(r.upper[...], 0.0)
        r.hidden[...] = (upper * upper).astype(jnp.bfloat16)

    near = {}

    def go_down(s, u):
        product = jnp.zeros((count, columns), jnp.float32)
        for p in range(pieces):
            loads_down[s, u, p].wait()
            product = product + jnp.dot(
                r.hidden[:, p * depth_down : (p + 1) * depth_down],
                r.down[(s * t + u) * pieces + p],
                preferred_element_type=jnp.float32,
            )
        if u:
            r.near_sent[s, u - 1] = product.astype(jnp.bfloat16)
            near[s, u] = send(
                r.near_sent.at[s, u - 1],
                r.near_got.at[s, u - 1],
                r.near_send.at[s, u - 1],
                r.near_recv.at[s, u - 1],
                at(0, u),
            )
        else:
            r.kept[s] = product

    def near_sum(s):
        value = r.kept[s]
        for u in range(1, t):
            near[s, u].wait_recv()
            value = value + r.near_got[s, u - 1].astype(jnp.float32)
        return value

    def far_copy(s, where):
        return pltpu.make_async_remote_copy(
            src_ref=r.far_sent.at[s],
            dst_ref=r.far_got.at[kv],
            send_sem=r.far_send.at[s],
            recv_sem=r.far_recv.at[kv],
            device_id={"kv": where, "tp": tp},
            device_id_type=MESH,
        )

    def far_relay():
        return pltpu.make_async_remote_copy(
            src_ref=r.far_sent.at[0],
            dst_ref=r.far_relay,
            send_sem=r.far_send.at[0],
            recv_sem=r.far_relay_recv,
            device_id={"kv": buddy, "tp": tp},
            device_id_type=MESH,
        )

    def far_out(s):
        value = near_sum(s)
        if relay and s == 0:
            r.far_sent[s] = value.astype(jnp.bfloat16)
            pl.when(is_end)(lambda: far_relay().start())
            pl.when(is_relay)(lambda: far_copy(s, dests[s]).start())
        elif relay and s == 2:
            r.kept[s] = value

            @pl.when(is_relay)
            def _():
                far_relay().wait_recv()
                r.kept[s] = r.kept[s] + r.far_relay[...].astype(jnp.float32)

            r.far_sent[s] = r.kept[s].astype(jnp.bfloat16)
            far_copy(s, dests[s]).start()
        else:
            r.far_sent[s] = value.astype(jnp.bfloat16)
            far_copy(s, dests[s]).start()

    def far_arrival(o):
        sender = shifted(kv, o, n)
        return pltpu.make_async_remote_copy(
            src_ref=r.far_sent.at[0],
            dst_ref=r.far_got.at[sender],
            send_sem=r.far_send.at[0],
            recv_sem=r.far_recv.at[sender],
            device_id={"kv": sender, "tp": tp},
            device_id_type=MESH,
        )

    def second_sum():
        second = residual_scale * r.own_normed[...].astype(jnp.float32) + near_sum(n - 1)
        for o in range(1, n):
            guarded(straight(o), far_arrival(o).wait_recv)
            second = second + r.far_got[shifted(kv, o, n)].astype(jnp.float32)
        r.kept[0] = second
        pending.extend(near.values())

    def second_norm():
        second = r.kept[0]
        sums = jnp.concatenate(
            [
                to_lanes(jnp.sum(second, axis=1, keepdims=True)),
                to_lanes(jnp.sum(second * second, axis=1, keepdims=True)),
            ],
            axis=0,
        )
        r.stats[0, 0:2] = sums
        tallies = []
        for i, (o, u) in enumerate(offsets):
            tallies.append(
                send(
                    r.stats.at[0],
                    r.stats.at[i + 1],
                    r.stats_send.at[i],
                    r.stats_recv.at[i],
                    at(o, u),
                )
            )
        pending.extend(tallies)
        for i, copy in enumerate(tallies):
            copy.wait_recv()
            sums = sums + r.stats[i + 1, 0:2]
        center_two = to_sublanes(sums[0:1]) / width
        spread_two = to_sublanes(sums[1:2]) / width - center_two * center_two
        result = (second - center_two) * lax.rsqrt(spread_two + epsilon)
        r.out[...] = (result * r.gain_two[...] + r.bias_two[...]).astype(jnp.bfloat16)

    def drain():
        for j in range(groups):
            finish_sends(j)
            finish_mixes(j)
        finish_firsts()
        for s in range(n - 1):
            far_copy(s, dests[s]).wait_send()
        for copy in pending:
            copy.wait_send()

    load_small([(r.tokens_in, r.tokens)])
    load_weights(0)
    greet_all()
    for c in range(1, groups // parts):
        load_weights(c)
    load_small(vectors)
    wait_tokens()
    for c in range(groups // parts):
        project(c)
        if c == 0:
            wait_barrier()
        for j in range(c * parts, (c + 1) * parts):
            send_far(j)
            send_near(j, is_relay if relay else None)
            if relay and j >= lag:
                send_near(j - lag, is_end)
            load_state(j)
    if relay:
        for j in range(max(groups - lag, 0), groups):
            send_near(j, is_end)
    load_rest()
    for j in range(lead):
        pass_relay(j)
    send_affine()
    fill()
    for j in range(groups):
        wait_sums(j)
        prepare(j)
        update(j)
        gated_out(j)
        if j + lead < groups:
            pass_relay(j + lead)
    for j in range(groups):
        forward_mixes(j)
    for j in range(groups):
        wait_mixes(j)
        project_out(j)
    pair_sum()
    tell_first()
    send_firsts()
    first_stats()
    go_up(0, 0, True)
    wait_first(arrivals[0], 0)
    forward()
    for u in range(1, t):
        wait_first(0, u)
        go_up(0, u, False)
    for i in range(n - 1):
        if i:
            wait_first(arrivals[i], 0)
        go_up(arrivals[i], 0, False)
        if i:
            for u in range(1, t):
                wait_first(arrivals[i - 1], u)
                go_up(arrivals[i - 1], u, False)
    for u in range(1, t):
        wait_first(arrivals[-1], u)
        go_up(arrivals[-1], u, False)
    square()
    for s in range(n):
        for u in range(1, t):
            go_down(s, u)
        if s:
            far_out(s - 1)
        go_down(s, 0)
    second_sum()
    second_norm()
    drain()


def layer(n, t, tokens, state, weights, bound, gain, w_out, w_up, w_down, affine):
    count, depth = tokens.shape
    rows = count // n
    width = weights[0].shape[1]
    kinds = len(weights)
    size = state.shape[3]
    lanes = 2 * size
    wide = min(width, GROUP_HEADS * size)
    span = min(width, 8 * size)
    groups = width // wide
    heads = wide // size
    columns = affine[0].shape[1]
    model, units = w_up.shape
    group = n * t
    up_width = min(units, 512)
    dma = pltpu.SemaphoreType.DMA
    vmem = pltpu.VMEM
    few, many = jnp.bfloat16, jnp.float32
    chunks = width // span * kinds
    shares = columns == span and units % depth == 0 and group * (units // depth) == chunks
    pieces = units // depth if shares else 1
    inputs = {
        "tokens_in": tokens,
        "state": state,
        "w_query": weights[0],
        "w_forget": weights[1],
        "w_input": weights[2],
        "w_gate": weights[3],
        "bound_in": bound,
        "gain_in": gain,
        "w_out": w_out,
        "w_up": w_up,
        "w_down": w_down,
        "gain_one_in": affine[0],
        "bias_one_in": affine[1],
        "gain_two_in": affine[2],
        "bias_two_in": affine[3],
    }
    scratch = {
        "tokens": vmem(tokens.shape, few),
        "bound": vmem(bound.shape, many),
        "gain": vmem(gain.shape, many),
        "gain_one": vmem((1, columns), many),
        "bias_one": vmem((1, columns), many),
        "gain_two": vmem((1, columns), many),
        "bias_two": vmem((1, columns), many),
        "pool": vmem((chunks, depth, span), few),
        "whole": vmem((groups, kinds, n, rows, wide), many),
        "sent": vmem((groups, n, kinds, rows, wide), few),
        "got": vmem((groups, 2 if n == 4 else n - 1, kinds, rows, wide), few),
        "relay_got": vmem((groups, 2, kinds, rows, wide), few),
        "relay_sent": vmem((groups, 2, kinds, rows, wide), few),
        "pick": vmem((4 * rows, rows * 2 * lanes), few),
        "factors": vmem((heads, size, 4 * rows), few),
        "value": vmem((heads, rows, lanes), many),
        "gate": vmem((rows, wide), many),
        "spread": vmem((2, size, rows * 2 * lanes), many),
        "read": vmem((heads, rows, size), many),
        "gathered": vmem((groups, n, rows, wide), few),
        "out_buf": vmem((t, width, columns), few),
        "mixed": vmem((t, count, columns), many),
        "up_buf": vmem((units // up_width, model, up_width), few),
        "part_got": vmem((t - 1, count, columns), many),
        "affine": vmem((group, 2, columns), many),
        "firsts": vmem((group, count, columns), few),
        "tallies": vmem((group, 8, count), many),
        "center": vmem((count, 128), many),
        "scale": vmem((count, 128), many),
        "upper": vmem((count, units), many),
        "own_normed": vmem((count, columns), few),
        "hidden": vmem((count, units), few),
        "near_sent": vmem((n, t - 1, count, columns), few),
        "near_got": vmem((n, t - 1, count, columns), few),
        "kept": vmem((n, count, columns), many),
        "far_sent": vmem((n, count, columns), few),
        "far_got": vmem((n, count, columns), few),
        "far_relay": vmem((count, columns), few),
        "stats": vmem((group, 8, count), many),
        "small_sem": dma((7,)),
        "load_project": dma((chunks,)),
        "load_state": dma((groups,)),
        "load_out": dma((t,)),
        "load_up": dma((units // up_width,)),
        "load_down": dma((group * pieces,)),
        "sum_send": dma((groups, n - 1)),
        "sum_recv": dma((groups, n - 1)),
        "relay_send": dma((groups, 2)),
        "relay_recv": dma((groups, 2)),
        "forward_send": dma,
        "far_relay_recv": dma,
        "mix_send": dma((groups, n)),
        "mix_recv": dma((groups, n)),
        "mix_forward": dma((groups, 2)),
        "tally_send": dma((group,)),
        "tally_recv": dma((group,)),
        "part_send": dma((t,)),
        "part_recv": dma((t,)),
        "affine_send": dma((n, t)),
        "affine_recv": dma((n, t)),
        "first_send": dma((n, t)),
        "first_recv": dma((n, t)),
        "near_send": dma((n, t)),
        "near_recv": dma((n, t)),
        "far_send": dma((n,)),
        "far_recv": dma((n,)),
        "stats_send": dma((group,)),
        "stats_recv": dma((group,)),
    }
    if not shares:
        scratch["down"] = vmem((group, units, columns), few)

    def kernel(*refs):
        names = [*inputs, "out", "new_state", *scratch]
        if shares:
            names.append("down")
            refs = (*refs, refs[names.index("pool")])
        layer_kernel(n, t, size, names, *refs)

    return pl.pallas_call(
        kernel,
        out_shape=(vmem((count, columns), few), vmem(state.shape, many)),
        in_specs=[pl.BlockSpec(memory_space=pl.ANY)] * len(inputs),
        out_specs=(pl.BlockSpec(memory_space=pltpu.VMEM),) * 2,
        scratch_shapes=list(scratch.values()),
        compiler_params=pltpu.CompilerParams(
            collective_id=0, has_side_effects=True, vmem_limit_bytes=LAYER_BYTES
        ),
        name="layer",
    )(*inputs.values())


def write_kernel(result, new_state, result_out, state_out, sem):
    pieces = sem.shape[0] - 1
    heads = new_state.shape[1] // pieces
    copies = [store(result, result_out, sem.at[pieces])]
    for i in range(pieces):
        part = pl.ds(i * heads, heads)
        copies.append(store(new_state.at[:, part], state_out.at[:, part], sem.at[i]))
    for copy in copies:
        copy.wait()


def write_out(result, new_state):
    return pl.pallas_call(
        write_kernel,
        out_shape=(
            jax.ShapeDtypeStruct(result.shape, result.dtype),
            jax.ShapeDtypeStruct(new_state.shape, new_state.dtype),
        ),
        in_specs=[pl.BlockSpec(memory_space=pltpu.VMEM)] * 2,
        out_specs=(pl.BlockSpec(memory_space=pl.ANY),) * 2,
        scratch_shapes=[pltpu.SemaphoreType.DMA((9,))],
        compiler_params=pltpu.CompilerParams(vmem_limit_bytes=WRITE_BYTES),
        name="write",
    )(result, new_state)


def per_device(
    tokens,
    state,
    w_query,
    w_forget,
    w_input,
    w_gate,
    lower_bound,
    head_gain,
    w_out,
    gain_one,
    bias_one,
    w_up,
    w_down,
    gain_two,
    bias_two,
):
    n, t = lax.axis_size("kv"), lax.axis_size("tp")
    result, new_state = layer(
        n,
        t,
        tokens,
        state,
        (w_query, w_forget, w_input, w_gate),
        lower_bound[None, :],
        head_gain[None, :],
        w_out,
        w_up,
        w_down,
        [vector[None, :] for vector in (gain_one, bias_one, gain_two, bias_two)],
    )
    return write_out(result, new_state)


def solution(mesh):
    placed = (
        P("dp", "kv"),
        P(("dp", "kv"), "tp", None, None),
        P("kv", "tp"),
        P("kv", "tp"),
        P("kv", "tp"),
        P("kv", "tp"),
        P("tp"),
        P(),
        P("tp", "kv"),
        P(("kv", "tp")),
        P(("kv", "tp")),
        P(None, ("kv", "tp")),
        P(("kv", "tp"), None),
        P(("kv", "tp")),
        P(("kv", "tp")),
    )
    return jax.shard_map(
        per_device,
        mesh=mesh,
        in_specs=placed,
        out_specs=(P("dp", ("kv", "tp")), P(("dp", "kv"), "tp", None, None)),
        check_vma=False,
    )
```

```python
import functools
import types

import jax
import jax.numpy as jnp
import numpy as np
from jax import lax
from jax.experimental import pallas as pl
from jax.experimental.pallas import tpu as pltpu
from jax.sharding import PartitionSpec as P

epsilon = 0.1
residual_scale = 1.68
MESH = pl.DeviceIdType.MESH
LAYER_BYTES = 47 * 1024 * 1024
WRITE_BYTES = 1024 * 1024
GROUP_HEADS = 4
LAG = 3
LEAD = 5


def shifted(index, by, count):
    return lax.rem(index + by, count)


def greet(peers):
    barrier = pltpu.get_barrier_semaphore()
    for peer in peers:
        pl.semaphore_signal(barrier, inc=1, device_id=peer, device_id_type=MESH)
    return lambda: pl.semaphore_wait(barrier, len(peers))


def send(source, target, send_sem, recv_sem, peer):
    copy = pltpu.make_async_remote_copy(
        src_ref=source,
        dst_ref=target,
        send_sem=send_sem,
        recv_sem=recv_sem,
        device_id=peer,
        device_id_type=MESH,
    )
    copy.start()
    return copy


def store(source, target, sem):
    copy = pltpu.make_async_copy(source, target, sem)
    copy.start()
    return copy


def to_lanes(column):
    count = column.shape[0]
    diagonal = lax.broadcasted_iota(jnp.int32, (count, count), 0) == lax.broadcasted_iota(
        jnp.int32, (count, count), 1
    )
    return jnp.sum(jnp.where(diagonal, column, 0.0), axis=0, keepdims=True)


def to_sublanes(row):
    count = row.shape[1]
    diagonal = lax.broadcasted_iota(jnp.int32, (count, count), 0) == lax.broadcasted_iota(
        jnp.int32, (count, count), 1
    )
    return jnp.sum(jnp.where(diagonal, row, 0.0), axis=1, keepdims=True)


def fill_pick(pick, rows, lanes):
    shape = (4 * rows, 2 * lanes)
    line = lax.broadcasted_iota(jnp.int32, shape, 0)
    lane = lax.broadcasted_iota(jnp.int32, shape, 1)
    same_half = (line < 2 * rows) == (lane < lanes)
    row = lax.rem(line, rows)
    for b in range(rows):
        chosen = jnp.where(same_half & (row == b), 1.0, 0.0)
        pick[:, b * 2 * lanes : (b + 1) * 2 * lanes] = chosen.astype(jnp.bfloat16)


def layer_kernel(n, t, size, names, *refs):
    r = types.SimpleNamespace(**dict(zip(names, refs)))
    kv, tp = lax.axis_index("kv"), lax.axis_index("tp")
    count, columns = r.out.shape
    rows = count // n
    group = n * t
    me = kv * t + tp
    width = group * columns
    groups, kinds, _, _, wide = r.whole.shape
    heads = wide // size
    lanes = 2 * size
    pieces = r.down.shape[0] // group
    depth_down = r.down.shape[1]
    offsets = [(o, u) for o in range(n) for u in range(t) if (o, u) != (0, 0)]
    relay = n == 4
    buddy = kv + 1 - 2 * lax.rem(kv, 2)

    def at(o, u):
        return {"kv": shifted(kv, o, n), "tp": shifted(tp, u, t)}

    def block(o, u):
        return shifted(kv, o, n) * t + shifted(tp, u, t)

    arrivals = sorted(range(1, n), key=lambda o: min(o, n - o))
    if relay:
        arrivals = [2, 3 - 2 * (kv // 2), 1 + 2 * (kv // 2)]

    def columns_of(index):
        return pl.ds(pl.multiple_of(index * columns, columns), columns)

    barrier = pltpu.get_barrier_semaphore()

    def greet_all():
        for o, u in offsets:
            pl.semaphore_signal(barrier, inc=1, device_id=at(o, u), device_id_type=MESH)

    def wait_barrier():
        pl.semaphore_wait(barrier, len(offsets))

    small = []

    def load_small(pairs):
        for source, target in pairs:
            small.append(store(source, target, r.small_sem.at[len(small)]))

    weights = (r.w_query, r.w_forget, r.w_input, r.w_gate)
    loads = {}

    span = r.pool.shape[2]
    parts = span // wide
    extra = r.scaled.shape[1] - count

    def load_weights(c):
        for w in range(kinds):
            loads[c, w] = store(
                weights[w].at[:, pl.ds(c * span, span)],
                r.pool.at[c * kinds + w],
                r.load_project.at[c * kinds + w],
            )

    def wait_tokens():
        small[0].wait()

    def fill():
        fill_pick(r.pick, rows, lanes)
        if relay:

            @pl.when(is_end)
            def _():
                r.far_got[3 - kv] = jnp.zeros(r.far_got.shape[1:], jnp.bfloat16)

    def guarded(condition, action):
        if condition is None:
            action()
        else:
            pl.when(condition)(action)

    def direct(j, o):
        slot = 1 if relay else o - 1
        where = buddy if relay else shifted(kv, o, n)
        return pltpu.make_async_remote_copy(
            src_ref=r.sent.at[j, where],
            dst_ref=r.got.at[j, slot],
            send_sem=r.sum_send.at[j, slot],
            recv_sem=r.sum_recv.at[j, slot],
            device_id={"kv": where, "tp": tp},
            device_id_type=MESH,
        )

    reach = (1,) if relay else tuple(range(1, n))

    vectors = [
        (r.bound_in, r.bound),
        (r.gain_in, r.gain),
        (r.gain_one_in, r.gain_one),
        (r.bias_one_in, r.bias_one),
        (r.gain_two_in, r.gain_two),
        (r.bias_two_in, r.bias_two),
    ]
    is_end = (kv == 0) | (kv == n - 1)
    is_relay = (kv != 0) & (kv != n - 1)
    lag = LAG
    lead = min(LEAD, groups)

    def to_relay(j, i):
        return pltpu.make_async_remote_copy(
            src_ref=r.sent.at[j, 3 - (buddy if i else kv)],
            dst_ref=r.relay_got.at[j, i],
            send_sem=r.relay_send.at[j, i],
            recv_sem=r.relay_recv.at[j, i],
            device_id={"kv": buddy, "tp": tp},
            device_id_type=MESH,
        )

    def from_relay(j, i):
        target = 3 - (kv if i else buddy)
        return target, pltpu.make_async_remote_copy(
            src_ref=r.relay_sent.at[j, i],
            dst_ref=r.got.at[j, 0],
            send_sem=r.relay_send.at[j, i],
            recv_sem=r.sum_recv.at[j, 0],
            device_id={"kv": target, "tp": tp},
            device_id_type=MESH,
        )

    def project(c):
        for w in range(kinds):
            loads[c, w].wait()
            value = jnp.dot(
                r.tokens[...], r.pool[c * kinds + w], preferred_element_type=jnp.float32
            ).reshape(n, rows, span)
            for p in range(parts):
                here = value[:, :, p * wide : (p + 1) * wide]
                r.whole[c * parts + p, w] = here
                r.sent[c * parts + p, :, w] = here.astype(jnp.bfloat16)

    def send_far(j):
        if relay:

            @pl.when(is_end)
            def _():
                for i in range(2):
                    to_relay(j, i).start()

    def send_near(j, chosen):
        def start():
            for o in reach:
                direct(j, o).start()

        guarded(chosen, start)

    def pass_relay(j):
        if not relay:
            return

        @pl.when(is_relay)
        def _():
            for i in range(2):
                to_relay(j, i).wait_recv()
                target, copy = from_relay(j, i)
                for w in range(kinds):
                    total = r.whole[j, w, target] + r.relay_got[j, i, w].astype(jnp.float32)
                    r.relay_sent[j, i, w] = total.astype(jnp.bfloat16)
                copy.start()

    def finish_sends(j):
        for o in reach:
            direct(j, o).wait_send()
        if relay:
            for i in range(2):
                to_relay(j, i).wait_send()

    def load_state(j):
        part = pl.ds(j * heads, heads)
        state_loads[j] = store(r.state.at[:, part], r.new_state.at[:, part], r.load_state.at[j])

    pending = []

    def wait_sums(j):
        if relay:
            from_relay(j, 0)[1].wait_recv()
        for o in reach:
            direct(j, o).wait_recv()

    def prepare(j):
        def summed(w):
            total = r.whole[j, w, kv]
            for slot in range(r.got.shape[1]):
                total = total + r.got[j, slot, w].astype(jnp.float32)
            return total.astype(jnp.bfloat16).astype(jnp.float32)

        query_raw, forget_raw, value, gate = (summed(w) for w in range(kinds))
        low = r.bound[:, j * wide : (j + 1) * wide]
        forget = low + (1.0 - low) * jax.nn.sigmoid(forget_raw)
        query = query_raw * jax.nn.sigmoid(query_raw)
        stacked = []
        for factor in (forget, query):
            high = factor.astype(jnp.bfloat16).astype(jnp.float32)
            stacked += [high, factor - high]
        turned = jnp.concatenate(stacked, axis=0).T.reshape(heads, size, 4 * rows)
        r.factors[...] = turned.astype(jnp.bfloat16)
        for h in range(heads):
            pair = value[:, (h // 2) * lanes : (h // 2 + 1) * lanes]
            r.value[h] = pltpu.roll(pair, size, 1) if h % 2 else pair
        r.gate[...] = gate * jax.nn.sigmoid(gate)

    def update(j):
        state_loads[j].wait()

        def one_head(h, slot):
            r.spread[slot] = jnp.dot(
                r.factors[h], r.pick[...], preferred_element_type=jnp.float32
            )
            for b in range(rows):
                base = b * 2 * lanes
                line = r.value[h, b : b + 1, :size]
                keep = r.spread[slot, :, base : base + size]
                query_column = r.spread[slot, :, base + lanes : base + lanes + size]
                updated = line + keep * (r.new_state[b, j * heads + h] - line)
                r.new_state[b, j * heads + h] = updated
                r.read[h, b : b + 1] = jnp.sum(updated * query_column, axis=0, keepdims=True)

        def two_heads(i, carry):
            for slot in range(2):
                one_head(i * 2 + slot, slot)
            return carry

        lax.fori_loop(0, heads // 2, two_heads, 0)

    def gated_out(j):
        def normalized(h):
            whole = r.read[h]
            return whole * lax.rsqrt(jnp.mean(whole * whole, axis=1, keepdims=True) + epsilon)

        gain = jnp.concatenate([r.gain[...]] * 2, axis=1)
        for p in range(heads // 2):
            here = slice(p * lanes, (p + 1) * lanes)
            pair = jnp.concatenate([normalized(2 * p), normalized(2 * p + 1)], axis=1)
            gated = pair * gain * r.gate[:, here]
            r.gathered[j, kv, :, here] = gated.astype(jnp.bfloat16)
        for o in range(1, n):
            guarded(sends_mix(j, o), mix_copy(j, o).start)

    def mix_copy(j, o):
        return pltpu.make_async_remote_copy(
            src_ref=r.gathered.at[j, kv],
            dst_ref=r.gathered.at[j, kv],
            send_sem=r.mix_send.at[j, o],
            recv_sem=r.mix_recv.at[j, o],
            device_id=at(o, 0),
            device_id_type=MESH,
        )

    def hops(j):
        return relay and j < groups - 2

    def sends_mix(j, o):
        return (kv != 3 if o == 1 else kv != 0 if o == 3 else is_relay) if hops(j) else None

    def forward_mix(j, i):
        return pltpu.make_async_remote_copy(
            src_ref=r.gathered.at[j, buddy],
            dst_ref=r.gathered.at[j, buddy],
            send_sem=r.mix_forward.at[j, i],
            recv_sem=r.mix_recv.at[j, 5 - 2 * kv if i else 2],
            device_id={"kv": 3 - (buddy if i else kv), "tp": tp},
            device_id_type=MESH,
        )

    def forward_mixes(j):
        if not hops(j):
            return

        @pl.when(is_relay)
        def _():
            pltpu.make_async_remote_copy(
                src_ref=r.gathered.at[j, kv],
                dst_ref=r.gathered.at[j, buddy],
                send_sem=r.mix_send.at[j, 1],
                recv_sem=r.mix_recv.at[j, 2 * kv - 1],
                device_id={"kv": buddy, "tp": tp},
                device_id_type=MESH,
            ).wait_recv()
            for i in range(2):
                forward_mix(j, i).start()

    def finish_mixes(j):
        for o in range(1, n):
            guarded(sends_mix(j, o), mix_copy(j, o).wait_send)
        if hops(j):

            @pl.when(is_relay)
            def _():
                for i in range(2):
                    forward_mix(j, i).wait_send()

    def wait_mixes(j):
        for o in range(1, n):
            condition = None
            if hops(j) and o != 2:
                condition = kv != (1 if o == 1 else 2)
            guarded(condition, mix_copy(j, o).wait_recv)

    def project_out(j):
        whole = r.gathered[j].reshape(count, wide)
        for u in range(t):
            if j == 0:
                loads_out[u].wait()
            product = jnp.dot(
                whole,
                r.out_buf[u, j * wide : (j + 1) * wide],
                preferred_element_type=jnp.float32,
            )
            r.mixed[u] = product if j == 0 else r.mixed[u] + product

    loads_out, loads_up, loads_down, state_loads = {}, {}, {}, {}
    up_chunks, _, up_width = r.up_buf.shape
    dests = [shifted(kv, o, n) for o in [*range(1, n), 0]]
    if relay:
        tables = [(3, 2, 1, 0), (2, 0, 3, 1), (1, 3, 0, 2), (0, 1, 2, 3)]
        dests = [
            jnp.where(kv < 2, jnp.where(kv == 0, a, b), jnp.where(kv == 2, c, d))
            for a, b, c, d in zip(*tables)
        ]

    def load_rest():
        for u in range(t):
            loads_out[u] = store(
                r.w_out.at[:, columns_of(shifted(tp, u, t))], r.out_buf.at[u], r.load_out.at[u]
            )
        for c in range(up_chunks):
            loads_up[c] = store(
                r.w_up.at[:, pl.ds(c * up_width, up_width)], r.up_buf.at[c], r.load_up.at[c]
            )
        for s in range(n):
            for u in [*range(1, t), 0]:
                for p in range(pieces):
                    slot = (s * t + u) * pieces + p
                    part = pl.ds(p * depth_down, depth_down)
                    loads_down[s, u, p] = store(
                        r.w_down.at[part, columns_of(dests[s] * t + shifted(tp, u, t))],
                        r.down.at[slot],
                        r.load_down.at[slot],
                    )

    affines = []

    def send_affine():
        for copy in small[1:]:
            copy.wait()
        r.affine[me, 0:1] = r.gain_one[...]
        r.affine[me, 1:2] = r.bias_one[...]
        for o, u in offsets:
            affines.append(
                send(
                    r.affine.at[me],
                    r.affine.at[me],
                    r.affine_send.at[o, u],
                    r.affine_recv.at[o, u],
                    at(o, u),
                )
            )
        pending.extend(affines)

    def pair_sum():
        parts = []
        for u in range(1, t):
            parts.append(
                send(
                    r.mixed.at[u],
                    r.part_got.at[u - 1],
                    r.part_send.at[u],
                    r.part_recv.at[u],
                    at(0, u),
                )
            )
        pending.extend(parts)
        own_tokens = r.tokens[:, columns_of(tp)].astype(jnp.float32)
        first = residual_scale * own_tokens + r.mixed[0]
        for u in range(1, t):
            parts[u - 1].wait_recv()
            first = first + r.part_got[u - 1]
        r.mixed[0] = first
        r.firsts[me] = first.astype(jnp.bfloat16)

    def hand_over(index, o, u, where):
        return pltpu.make_async_remote_copy(
            src_ref=r.firsts.at[index],
            dst_ref=r.firsts.at[index],
            send_sem=r.first_send.at[o, u],
            recv_sem=r.first_recv.at[o, u],
            device_id=where,
            device_id_type=MESH,
        )

    def tell_first():
        first = r.mixed[0]
        total = jnp.sum(first, axis=1, keepdims=True)
        away = first - total / columns
        r.tallies[0, 0:2] = jnp.concatenate(
            [to_lanes(total), to_lanes(jnp.sum(away * away, axis=1, keepdims=True))], axis=0
        )
        for i, (o, u) in enumerate(offsets):
            counts.append(
                send(
                    r.tallies.at[0],
                    r.tallies.at[i + 1],
                    r.tally_send.at[i],
                    r.tally_recv.at[i],
                    at(o, u),
                )
            )
        pending.extend(counts)

    counts = []
    def straight(o):
        return (kv != 0 if o == 3 else kv != 3) if relay and o != 2 else None

    def send_firsts():
        for u in range(1, t):
            copy = hand_over(me, 0, u, at(0, u))
            copy.start()
            pending.append(copy)
        for o in sorted(range(1, n), key=lambda o: -min(o, n - o)):
            copy = hand_over(me, o, 0, at(o, 0))
            guarded(straight(o), copy.start)

    def forward_first():
        return pltpu.make_async_remote_copy(
            src_ref=r.firsts.at[block(2, 0)],
            dst_ref=r.firsts.at[block(2, 0)],
            send_sem=r.forward_send,
            recv_sem=r.first_recv.at[2 * kv - 1, 0],
            device_id={"kv": buddy, "tp": tp},
            device_id_type=MESH,
        )

    def finish_firsts():
        for o in range(1, n):
            guarded(straight(o), hand_over(me, o, 0, at(o, 0)).wait_send)
        if relay:
            pl.when(is_relay)(lambda: forward_first().wait_send())

    def first_stats():
        for copy in counts:
            copy.wait_recv()
        tallies = [r.tallies[i, 0:2] for i in range(group)]
        center = sum(tally[0:1] for tally in tallies) / width
        spread = jnp.zeros_like(center)
        for tally in tallies:
            away = tally[0:1] / columns - center
            spread = spread + tally[1:2] + columns * (away * away)
        scale = lax.rsqrt(spread / width + epsilon)
        r.center[...] = jnp.broadcast_to(to_sublanes(center), r.center.shape)
        r.scale[...] = jnp.broadcast_to(to_sublanes(scale), r.scale.shape)

    def wait_first(o, u):
        hand_over(block(n - o, 0), o, u, at(0, u)).wait_recv()
        if u == 0:
            for v in range(1, t):
                copy = hand_over(block(n - o, 0), o, v, at(0, v))
                copy.start()
                pending.append(copy)

    def forward():
        if relay:
            pl.when(is_relay)(lambda: forward_first().start())

    def stack_affine():
        for copy in affines:
            copy.wait_recv()
        for g in range(group):
            pair = r.affine[g]
            high = pair.astype(jnp.bfloat16).astype(jnp.float32)
            lines = [high, pair - high, jnp.zeros((extra - 4, columns), jnp.float32)]
            r.scaled[g, count:] = jnp.concatenate(lines, axis=0).astype(jnp.bfloat16)

    def go_up(o, u, first_one):
        index = block(n - o, t - u)
        gain = r.affine[index, 0:1]
        r.scaled[index, :count] = (r.firsts[index].astype(jnp.float32) * gain).astype(jnp.bfloat16)
        for c in range(up_chunks):
            here = slice(c * up_width, (c + 1) * up_width)
            if first_one:
                loads_up[c].wait()
            product = jnp.dot(
                r.scaled[index],
                r.up_buf[c, columns_of(index)],
                preferred_element_type=jnp.float32,
            )
            r.upper[:, here] = product if first_one else r.upper[:, here] + product

    def square():
        center, scale = r.center[:, 0:1], r.scale[:, 0:1]
        for c in range(up_chunks):
            here = slice(c * up_width, (c + 1) * up_width)
            tail = r.upper[count : count + 4, here]
            gain, bias = tail[0:1] + tail[2:3], tail[1:2] + tail[3:4]
            upper = jnp.maximum((r.upper[:count, here] - center * gain) * scale + bias, 0.0)
            r.hidden[:, here] = (upper * upper).astype(jnp.bfloat16)
        pair = r.affine[me]
        away = r.firsts[me].astype(jnp.float32) - center
        r.own_normed[...] = (away * scale * pair[0:1] + pair[1:2]).astype(jnp.bfloat16)

    near = {}

    def go_down(s, u):
        product = jnp.zeros((count, columns), jnp.float32)
        for p in range(pieces):
            loads_down[s, u, p].wait()
            product = product + jnp.dot(
                r.hidden[:, p * depth_down : (p + 1) * depth_down],
                r.down[(s * t + u) * pieces + p],
                preferred_element_type=jnp.float32,
            )
        if u:
            r.near_sent[s, u - 1] = product.astype(jnp.bfloat16)
            near[s, u] = send(
                r.near_sent.at[s, u - 1],
                r.near_got.at[s, u - 1],
                r.near_send.at[s, u - 1],
                r.near_recv.at[s, u - 1],
                at(0, u),
            )
        else:
            r.kept[s] = product

    def near_sum(s):
        value = r.kept[s]
        for u in range(1, t):
            near[s, u].wait_recv()
            value = value + r.near_got[s, u - 1].astype(jnp.float32)
        return value

    def far_copy(s, where):
        return pltpu.make_async_remote_copy(
            src_ref=r.far_sent.at[s],
            dst_ref=r.far_got.at[kv],
            send_sem=r.far_send.at[s],
            recv_sem=r.far_recv.at[kv],
            device_id={"kv": where, "tp": tp},
            device_id_type=MESH,
        )

    def far_relay():
        return pltpu.make_async_remote_copy(
            src_ref=r.far_sent.at[0],
            dst_ref=r.far_relay,
            send_sem=r.far_send.at[0],
            recv_sem=r.far_relay_recv,
            device_id={"kv": buddy, "tp": tp},
            device_id_type=MESH,
        )

    def far_out(s):
        value = near_sum(s)
        if relay and s == 0:
            r.far_sent[s] = value.astype(jnp.bfloat16)
            pl.when(is_end)(lambda: far_relay().start())
            pl.when(is_relay)(lambda: far_copy(s, dests[s]).start())
        elif relay and s == 2:
            r.kept[s] = value

            @pl.when(is_relay)
            def _():
                far_relay().wait_recv()
                r.kept[s] = r.kept[s] + r.far_relay[...].astype(jnp.float32)

            r.far_sent[s] = r.kept[s].astype(jnp.bfloat16)
            far_copy(s, dests[s]).start()
        else:
            r.far_sent[s] = value.astype(jnp.bfloat16)
            far_copy(s, dests[s]).start()

    def far_arrival(o):
        sender = shifted(kv, o, n)
        return pltpu.make_async_remote_copy(
            src_ref=r.far_sent.at[0],
            dst_ref=r.far_got.at[sender],
            send_sem=r.far_send.at[0],
            recv_sem=r.far_recv.at[sender],
            device_id={"kv": sender, "tp": tp},
            device_id_type=MESH,
        )

    def second_sum():
        second = residual_scale * r.own_normed[...].astype(jnp.float32) + near_sum(n - 1)
        for o in range(1, n):
            guarded(straight(o), far_arrival(o).wait_recv)
            second = second + r.far_got[shifted(kv, o, n)].astype(jnp.float32)
        r.kept[0] = second
        pending.extend(near.values())

    def second_norm():
        second = r.kept[0]
        sums = jnp.concatenate(
            [
                to_lanes(jnp.sum(second, axis=1, keepdims=True)),
                to_lanes(jnp.sum(second * second, axis=1, keepdims=True)),
            ],
            axis=0,
        )
        r.stats[0, 0:2] = sums
        tallies = []
        for i, (o, u) in enumerate(offsets):
            tallies.append(
                send(
                    r.stats.at[0],
                    r.stats.at[i + 1],
                    r.stats_send.at[i],
                    r.stats_recv.at[i],
                    at(o, u),
                )
            )
        pending.extend(tallies)
        for i, copy in enumerate(tallies):
            copy.wait_recv()
            sums = sums + r.stats[i + 1, 0:2]
        center_two = to_sublanes(sums[0:1]) / width
        spread_two = to_sublanes(sums[1:2]) / width - center_two * center_two
        result = (second - center_two) * lax.rsqrt(spread_two + epsilon)
        r.out[...] = (result * r.gain_two[...] + r.bias_two[...]).astype(jnp.bfloat16)

    def drain():
        for j in range(groups):
            finish_sends(j)
            finish_mixes(j)
        finish_firsts()
        for s in range(n - 1):
            far_copy(s, dests[s]).wait_send()
        for copy in pending:
            copy.wait_send()

    load_small([(r.tokens_in, r.tokens)])
    load_weights(0)
    greet_all()
    for c in range(1, groups // parts):
        load_weights(c)
    load_small(vectors)
    wait_tokens()
    for c in range(groups // parts):
        project(c)
        if c == 0:
            wait_barrier()
        for j in range(c * parts, (c + 1) * parts):
            send_far(j)
            send_near(j, is_relay if relay else None)
            if relay and j >= lag:
                send_near(j - lag, is_end)
            load_state(j)
    if relay:
        for j in range(max(groups - lag, 0), groups):
            send_near(j, is_end)
    load_rest()
    for j in range(lead):
        pass_relay(j)
    send_affine()
    fill()
    for j in range(groups):
        wait_sums(j)
        prepare(j)
        update(j)
        gated_out(j)
        if j + lead < groups:
            pass_relay(j + lead)
    for j in range(groups):
        forward_mixes(j)
    stack_affine()
    for j in range(groups):
        wait_mixes(j)
        project_out(j)
    pair_sum()
    send_firsts()
    tell_first()
    go_up(0, 0, True)
    for u in range(1, t):
        wait_first(0, u)
        go_up(0, u, False)
    wait_first(arrivals[0], 0)
    forward()
    go_up(arrivals[0], 0, False)
    for i in range(1, n - 1):
        wait_first(arrivals[i], 0)
        go_up(arrivals[i], 0, False)
        for u in range(1, t):
            wait_first(arrivals[i - 1], u)
            go_up(arrivals[i - 1], u, False)
    first_stats()
    for u in range(1, t):
        wait_first(arrivals[-1], u)
        go_up(arrivals[-1], u, False)
    square()
    for s in range(n):
        for u in range(1, t):
            go_down(s, u)
        if s:
            far_out(s - 1)
        go_down(s, 0)
    second_sum()
    second_norm()
    drain()


def layer(n, t, tokens, state, weights, bound, gain, w_out, w_up, w_down, affine):
    count, depth = tokens.shape
    rows = count // n
    width = weights[0].shape[1]
    kinds = len(weights)
    size = state.shape[3]
    lanes = 2 * size
    wide = min(width, GROUP_HEADS * size)
    span = min(width, 8 * size)
    groups = width // wide
    heads = wide // size
    columns = affine[0].shape[1]
    model, units = w_up.shape
    group = n * t
    up_width = min(units, 512)
    dma = pltpu.SemaphoreType.DMA
    vmem = pltpu.VMEM
    few, many = jnp.bfloat16, jnp.float32
    chunks = width // span * kinds
    shares = columns == span and units % depth == 0 and group * (units // depth) == chunks
    pieces = units // depth if shares else 1
    inputs = {
        "tokens_in": tokens,
        "state": state,
        "w_query": weights[0],
        "w_forget": weights[1],
        "w_input": weights[2],
        "w_gate": weights[3],
        "bound_in": bound,
        "gain_in": gain,
        "w_out": w_out,
        "w_up": w_up,
        "w_down": w_down,
        "gain_one_in": affine[0],
        "bias_one_in": affine[1],
        "gain_two_in": affine[2],
        "bias_two_in": affine[3],
    }
    scratch = {
        "tokens": vmem(tokens.shape, few),
        "bound": vmem(bound.shape, many),
        "gain": vmem(gain.shape, many),
        "gain_one": vmem((1, columns), many),
        "bias_one": vmem((1, columns), many),
        "gain_two": vmem((1, columns), many),
        "bias_two": vmem((1, columns), many),
        "pool": vmem((chunks, depth, span), few),
        "whole": vmem((groups, kinds, n, rows, wide), many),
        "sent": vmem((groups, n, kinds, rows, wide), few),
        "got": vmem((groups, 2 if n == 4 else n - 1, kinds, rows, wide), few),
        "relay_got": vmem((groups, 2, kinds, rows, wide), few),
        "relay_sent": vmem((groups, 2, kinds, rows, wide), few),
        "pick": vmem((4 * rows, rows * 2 * lanes), few),
        "factors": vmem((heads, size, 4 * rows), few),
        "value": vmem((heads, rows, lanes), many),
        "gate": vmem((rows, wide), many),
        "spread": vmem((2, size, rows * 2 * lanes), many),
        "read": vmem((heads, rows, size), many),
        "gathered": vmem((groups, n, rows, wide), few),
        "out_buf": vmem((t, width, columns), few),
        "mixed": vmem((t, count, columns), many),
        "up_buf": vmem((units // up_width, model, up_width), few),
        "part_got": vmem((t - 1, count, columns), many),
        "affine": vmem((group, 2, columns), many),
        "firsts": vmem((group, count, columns), few),
        "tallies": vmem((group, 8, count), many),
        "center": vmem((count, 128), many),
        "scale": vmem((count, 128), many),
        "scaled": vmem((group, count + 16, columns), few),
        "upper": vmem((count + 16, units), many),
        "own_normed": vmem((count, columns), few),
        "hidden": vmem((count, units), few),
        "near_sent": vmem((n, t - 1, count, columns), few),
        "near_got": vmem((n, t - 1, count, columns), few),
        "kept": vmem((n, count, columns), many),
        "far_sent": vmem((n, count, columns), few),
        "far_got": vmem((n, count, columns), few),
        "far_relay": vmem((count, columns), few),
        "stats": vmem((group, 8, count), many),
        "small_sem": dma((7,)),
        "load_project": dma((chunks,)),
        "load_state": dma((groups,)),
        "load_out": dma((t,)),
        "load_up": dma((units // up_width,)),
        "load_down": dma((group * pieces,)),
        "sum_send": dma((groups, n - 1)),
        "sum_recv": dma((groups, n - 1)),
        "relay_send": dma((groups, 2)),
        "relay_recv": dma((groups, 2)),
        "forward_send": dma,
        "far_relay_recv": dma,
        "mix_send": dma((groups, n)),
        "mix_recv": dma((groups, n)),
        "mix_forward": dma((groups, 2)),
        "tally_send": dma((group,)),
        "tally_recv": dma((group,)),
        "part_send": dma((t,)),
        "part_recv": dma((t,)),
        "affine_send": dma((n, t)),
        "affine_recv": dma((n, t)),
        "first_send": dma((n, t)),
        "first_recv": dma((n, t)),
        "near_send": dma((n, t)),
        "near_recv": dma((n, t)),
        "far_send": dma((n,)),
        "far_recv": dma((n,)),
        "stats_send": dma((group,)),
        "stats_recv": dma((group,)),
    }
    if not shares:
        scratch["down"] = vmem((group, units, columns), few)

    def kernel(*refs):
        names = [*inputs, "out", "new_state", *scratch]
        if shares:
            names.append("down")
            refs = (*refs, refs[names.index("pool")])
        layer_kernel(n, t, size, names, *refs)

    return pl.pallas_call(
        kernel,
        out_shape=(vmem((count, columns), few), vmem(state.shape, many)),
        in_specs=[pl.BlockSpec(memory_space=pl.ANY)] * len(inputs),
        out_specs=(pl.BlockSpec(memory_space=pltpu.VMEM),) * 2,
        scratch_shapes=list(scratch.values()),
        compiler_params=pltpu.CompilerParams(
            collective_id=0, has_side_effects=True, vmem_limit_bytes=LAYER_BYTES
        ),
        name="layer",
    )(*inputs.values())


def write_kernel(result, new_state, result_out, state_out, sem):
    pieces = sem.shape[0] - 1
    heads = new_state.shape[1] // pieces
    copies = [store(result, result_out, sem.at[pieces])]
    for i in range(pieces):
        part = pl.ds(i * heads, heads)
        copies.append(store(new_state.at[:, part], state_out.at[:, part], sem.at[i]))
    for copy in copies:
        copy.wait()


def write_out(result, new_state):
    return pl.pallas_call(
        write_kernel,
        out_shape=(
            jax.ShapeDtypeStruct(result.shape, result.dtype),
            jax.ShapeDtypeStruct(new_state.shape, new_state.dtype),
        ),
        in_specs=[pl.BlockSpec(memory_space=pltpu.VMEM)] * 2,
        out_specs=(pl.BlockSpec(memory_space=pl.ANY),) * 2,
        scratch_shapes=[pltpu.SemaphoreType.DMA((9,))],
        compiler_params=pltpu.CompilerParams(vmem_limit_bytes=WRITE_BYTES),
        name="write",
    )(result, new_state)


def per_device(
    tokens,
    state,
    w_query,
    w_forget,
    w_input,
    w_gate,
    lower_bound,
    head_gain,
    w_out,
    gain_one,
    bias_one,
    w_up,
    w_down,
    gain_two,
    bias_two,
):
    n, t = lax.axis_size("kv"), lax.axis_size("tp")
    result, new_state = layer(
        n,
        t,
        tokens,
        state,
        (w_query, w_forget, w_input, w_gate),
        lower_bound[None, :],
        head_gain[None, :],
        w_out,
        w_up,
        w_down,
        [vector[None, :] for vector in (gain_one, bias_one, gain_two, bias_two)],
    )
    return write_out(result, new_state)


def solution(mesh):
    placed = (
        P("dp", "kv"),
        P(("dp", "kv"), "tp", None, None),
        P("kv", "tp"),
        P("kv", "tp"),
        P("kv", "tp"),
        P("kv", "tp"),
        P("tp"),
        P(),
        P("tp", "kv"),
        P(("kv", "tp")),
        P(("kv", "tp")),
        P(None, ("kv", "tp")),
        P(("kv", "tp"), None),
        P(("kv", "tp")),
        P(("kv", "tp")),
    )
    return jax.shard_map(
        per_device,
        mesh=mesh,
        in_specs=placed,
        out_specs=(P("dp", ("kv", "tp")), P(("dp", "kv"), "tp", None, None)),
        check_vma=False,
    )
```
